32 devices in a mesh: sp: 4 (over z), dp: 8 (over y, x, core).
Axes of the slice: x: 2, y: 2, z: 4, core: 2. Of those that a mesh axis runs over, the one named last changes fastest.
Arguments:
- value_half: bfloat16 [8, 1536, 2048], P('dp', 'sp'), may hold values from -6 to 6
- gate_half: bfloat16 [8, 1536, 2048], P('dp', 'sp'), may hold values from -9 to 9
- conv_taps: bfloat16 [31, 2048], replicated, may hold values from -1 to 1
- norm_gain: float32 [2048], replicated, may hold values from 0.1 to 1.9
- norm_shift: float32 [2048], replicated, may hold values from -3 to 3
- out_weight: bfloat16 [2048, 2048], P('dp', 'sp'), may hold values from -0.125 to 0.125
Outputs:
- module_out: bfloat16 [8, 1536, 2048], P('dp', 'sp')
The draws below stay inside these ranges and needn't reach their ends.
All inputs are finite; a program needn't handle non-finite values.
Results may differ from the reference program's by a relative error of at most 0.0064.
Values may be sent and summed in bfloat16 or wider, within the bound.
A program may use at most 64 MiB of HBM per device.

```python
import jax
import jax.numpy as jnp
from jax import lax

D = 2048
CONV_W = 31
SEQ_LEN = 1536
SEQS = 8


def steps_of(stream_key, shape, shards, least, top_value):
    factor_of, own = 1.0, jax.random.fold_in(stream_key, 6)
    for position, shards_of in shards:
        heights = jnp.exp(jax.random.uniform(jax.random.fold_in(own, position), (shards_of,), jnp.float32, least / len(shards), top_value / len(shards)))
        factor_of = factor_of * jnp.repeat(heights, shape[position] // shards_of).reshape([-1 if axis == position else 1 for axis in range(len(shape))])
    return factor_of


def noise(own_key, shape, scale, limit, pieces=(), kind=jnp.bfloat16):
    values = jax.random.normal(own_key, shape, jnp.float32) * scale
    if len(pieces) > 0:
        values = steps_of(own_key, shape, pieces, -0.22, 0.18) * values
    return jnp.clip(values, min=-limit, max=limit).astype(kind)


def setup_inputs(seed: int = 0) -> dict:
    keys = jax.random.split(jax.random.key(seed), 7)
    value_half = noise(keys[0], (SEQS, SEQ_LEN, D), 1.0, 6.0, ((0, 8), (1, 4)))
    gate_half = noise(keys[1], (SEQS, SEQ_LEN, D), 1.5, 9.0, ((0, 8), (1, 4)))
    conv_taps = noise(keys[2], (CONV_W, D), CONV_W ** -0.5, 1.0)
    norm_gain = jnp.clip(1.0 + 0.18 * jax.random.normal(keys[3], (D,), jnp.float32), 0.1, 1.9)
    norm_shift = noise(keys[4], (D,), 0.5, 3.0, (), jnp.float32)
    out_weight = noise(keys[5], (D, D), D ** -0.5, 0.125, ((0, 8), (1, 4)))
    return {"value_half": value_half, "gate_half": gate_half, "conv_taps": conv_taps, "norm_gain": norm_gain, "norm_shift": norm_shift, "out_weight": out_weight}


EPSILON = 1e-06

def causal_mix(gated, conv_taps):
    tap_count = conv_taps.shape[0]
    length = gated.shape[0]
    padded = jnp.concatenate([jnp.zeros((tap_count - 1, gated.shape[1]), gated.dtype), gated], 0)
    running = jnp.zeros((length, gated.shape[1]), jnp.float32)
    for tap_index in range(tap_count):
        running = running + padded[tap_index:tap_index + length].astype(jnp.float32) * conv_taps[tap_index].astype(jnp.float32)
    return running.astype(jnp.bfloat16)

def one_sequence(pair, conv_taps, norm_gain, norm_shift, out_weight):
    value_rows, gate_rows = pair
    gated = (value_rows.astype(jnp.float32) * jax.nn.sigmoid(gate_rows.astype(jnp.float32))).astype(jnp.bfloat16)
    convolved = causal_mix(gated, conv_taps).astype(jnp.float32)
    mean_row = lax.optimization_barrier(jnp.mean(convolved, axis=-1, keepdims=True))
    centered = convolved - mean_row
    variance = lax.optimization_barrier(jnp.mean(centered * centered, axis=-1, keepdims=True))
    normed = centered * lax.rsqrt(variance + EPSILON) * norm_gain + norm_shift
    activated = jax.nn.silu(normed).astype(jnp.bfloat16)
    return jnp.dot(activated, out_weight, preferred_element_type=jnp.float32).astype(jnp.bfloat16)

def reference(value_half, gate_half, conv_taps, norm_gain, norm_shift, out_weight):
    return lax.map(lambda pair: one_sequence(pair, conv_taps, norm_gain, norm_shift, out_weight), (value_half, gate_half))
```

```python
import math

import jax
import jax.numpy as jnp
from jax import lax
from jax.experimental import pallas as pl
from jax.experimental.pallas import tpu as pltpu
from jax.sharding import PartitionSpec as P

EPSILON = 1e-06
MESH = pl.DeviceIdType.MESH
F32 = jnp.float32
BF16 = jnp.bfloat16
LANES = 128
VMEM_LIMIT = 62 * 1024 * 1024
ORDER = (
    "x0", "g0", "g1", "g2", "g3", "t0", "e0", "f0", "e1", "z1", "a0", "o1",
    "e2", "y0", "z2", "e3", "f1", "n0", "z3", "v0", "o2", "s0", "h0", "l0",
    "l1", "l2", "l3", "f2", "n1", "o3", "w1", "w2", "u1", "m0", "r0", "s1",
    "m1", "r1", "w3", "f3", "u2", "s2", "m2", "r2", "u3", "m3", "s3", "r3",
)


def half_sigmoid(x):
    return 0.5 * jnp.tanh(0.5 * x) + 0.5


def nearest(me, count, k):
    place = jnp.int32(0)
    for here in range(count):
        there = sorted(range(count), key=lambda j: (abs(j - here), j))[k]
        place = place + jnp.where(me == here, there, 0).astype(jnp.int32)
    return place


def make_kernel(sp, dp, xs, ys, parts, tok, width, taps, rows, cols, pad):
    group = sp // parts
    part_cols = group * cols
    late_rows = rows // 8 // 16 * 16 if group == 1 else 0
    half_rows = (rows - late_rows) // 2
    chips = xs * ys
    blocks = width // LANES
    row_chunk = 128 if tok % 128 == 0 else tok
    lead = pad - (taps - 1)
    in_parts = 4 if blocks % 4 == 0 else 1
    in_cols = width // in_parts
    streamed = rows % LANES == 0

    def kernel(v_hbm, g_hbm, taps_hbm, gain_hbm, shift_hbm, w_hbm, out_v,
               v_in, g_in, halo_v, halo_g, taps_in, taps_f, gain, shift, gated, conv, act, acc, wall,
               in_sem, halo_send, halo_recv, send_sem, z_send, z_sem, recv_sem, late_sem):
        s = lax.axis_index("sp")
        d = lax.axis_index("dp")
        core = lax.rem(d, 2)
        x = lax.rem(d // 2, xs)
        y = d // (2 * xs)

        def index(yy, xx, cc):
            return (yy * xs + xx) * 2 + cc

        sibling = index(y, x, 1 - core)

        def along_x(step):
            return lax.rem(x + step, xs)

        def along_y(step):
            return lax.rem(y + step, ys)

        own = wall.at[pl.ds(pl.multiple_of(d * rows, rows), rows), pl.ds(pl.multiple_of(s * cols, cols), cols)]
        w_copy = pltpu.make_async_copy(w_hbm, own, in_sem.at[0])
        w_copy.start()
        loads = []
        for part in range(in_parts):
            sl = pl.ds(part * in_cols, in_cols)
            pair = (
                pltpu.make_async_copy(v_hbm.at[0, :, sl], v_in.at[:, sl], in_sem.at[4 + 2 * part]),
                pltpu.make_async_copy(g_hbm.at[0, :, sl], g_in.at[:, sl], in_sem.at[5 + 2 * part]),
            )
            loads.append(pair)
            for copy in pair:
                copy.start()
        small = [
            pltpu.make_async_copy(taps_hbm, taps_in, in_sem.at[1]),
            pltpu.make_async_copy(gain_hbm, gain, in_sem.at[2]),
            pltpu.make_async_copy(shift_hbm, shift, in_sem.at[3]),
        ]
        for copy in small:
            copy.start()

        barrier = pltpu.get_barrier_semaphore()
        friends = [(s, sibling)]
        friends += [(s, index(y, along_x(i), core)) for i in range(1, xs)]
        friends += [(s, index(along_y(i), x, core)) for i in range(1, ys)]
        for friend in friends:
            pl.semaphore_signal(barrier, inc=1, device_id=friend, device_id_type=MESH)
        above, below = s + 1 < sp, s > 0

        @pl.when(above)
        def _():
            pl.semaphore_signal(barrier, inc=1, device_id=(lax.rem(s + 1, sp), d), device_id_type=MESH)

        @pl.when(below)
        def _():
            pl.semaphore_signal(barrier, inc=1, device_id=(lax.rem(s + sp - 1, sp), d), device_id_type=MESH)

        pl.semaphore_wait(barrier, len(friends) + above.astype(jnp.int32) + below.astype(jnp.int32))
        w_copy.wait()

        sent = []

        def send(region, sem, target):
            copy = pltpu.make_async_remote_copy(
                src_ref=region, dst_ref=region, send_sem=send_sem.at[len(sent)], recv_sem=sem,
                device_id=target, device_id_type=MESH)
            copy.start()
            sent.append(copy)

        def arrived(region, sem):
            pltpu.make_async_remote_copy(
                src_ref=region, dst_ref=region, send_sem=send_sem.at[0], recv_sem=sem,
                device_id=(s, sibling), device_id_type=MESH).wait_recv()

        def block(half, who):
            return wall.at[pl.ds(pl.multiple_of(d * rows + half * half_rows, 16), half_rows),
                           pl.ds(pl.multiple_of(who * cols, cols), cols)]

        def strip(half, dd, part):
            return wall.at[pl.ds(pl.multiple_of(dd * rows + half * half_rows, 16), half_rows),
                           pl.ds(pl.multiple_of(part * part_cols, part_cols), part_cols)]

        halo = [
            pltpu.make_async_remote_copy(
                src_ref=src.at[0, pl.ds(tok - pad, pad), :], dst_ref=dst, send_sem=halo_send.at[i],
                recv_sem=halo_recv.at[i], device_id=(lax.rem(s + 1, sp), d), device_id_type=MESH)
            for i, (src, dst) in enumerate(((v_hbm, halo_v), (g_hbm, halo_g)))
        ]

        def send_halo(i):
            @pl.when(s < sp - 1)
            def _():
                halo[i].start()

        guarded = []

        def send_if(wanted, region, sem, target, column=None):
            copy = pltpu.make_async_remote_copy(
                src_ref=region, dst_ref=region, send_sem=z_send.at[len(guarded)], recv_sem=sem,
                device_id=(target, d if column is None else column), device_id_type=MESH)

            @pl.when(wanted)
            def _():
                copy.start()

            guarded.append((wanted, copy))

        def z_sends():
            for half in range(2):
                send_if(s + 1 < sp, block(half, s), z_sem.at[half, s], lax.rem(s + 1, sp))
                send_if(s > 0, block(half, s), z_sem.at[half, s], lax.rem(s + sp - 1, sp))

        def z_link(k):
            source = nearest(s, sp, k)
            target = jnp.where(source < s, s + 1, s - 1)
            onward = jnp.logical_and(target >= 0, target < sp)
            return source, lax.rem(target + sp, sp), onward

        def z_forward(k):
            source, target, onward = z_link(k)
            for half in range(2):
                @pl.when(onward)
                def _():
                    arrived(block(half, source), z_sem.at[half, source])

                send_if(onward, block(half, source), z_sem.at[half, source], target)

        def z_last(k):
            source, _, onward = z_link(k)

            @pl.when(jnp.logical_not(onward))
            def _():
                for half in range(2):
                    arrived(block(half, source), z_sem.at[half, source])

        my_part = s // group
        part_of = [nearest(my_part, parts, k) for k in range(parts)]

        def firsts(half):
            if half == 0:
                return [index(y, along_x(i), core) for i in range(1, xs)]
            return [index(along_y(i), x, core) for i in range(1, ys)]

        def event_own(c):
            part = part_of[c]
            if group == 1 and c > 0:
                z_last(c)
            for half in range(2):
                for target in firsts(half):
                    send(strip(half, d, part), recv_sem.at[half, d, part], (s, target))
            for half in range(2):
                for target in firsts(1 - half):
                    send(strip(half, d, part), recv_sem.at[half, d, part], (s, target))
            for half in range(2):
                send(strip(half, d, part), recv_sem.at[half, d, part], (s, sibling))

        def event_first(c):
            part = part_of[c]
            for half in (1, 0):
                for dd in firsts(half):
                    region, sem = strip(half, dd, part), recv_sem.at[half, dd, part]
                    arrived(region, sem)
                    for target in firsts(1 - half):
                        send(region, sem, (s, target))
                    send(region, sem, (s, sibling))

        def event_second(c):
            part = part_of[c]
            for first in range(max(xs, ys)):
                for second in range(1, max(xs, ys)):
                    for half in range(2):
                        fx, fy = (first, second) if half == 0 else (second, first)
                        if fx >= xs or fy >= ys:
                            continue
                        dd = index(along_y(fy), along_x(fx), core)
                        region, sem = strip(half, dd, part), recv_sem.at[half, dd, part]
                        arrived(region, sem)
                        send(region, sem, (s, sibling))

        def late_strip(dd, who):
            return wall.at[pl.ds(pl.multiple_of(dd * rows + 2 * half_rows, 16), late_rows),
                           pl.ds(pl.multiple_of(who * cols, cols), cols)]

        def mine(i):
            return index(along_y(i // xs), along_x(i % xs), core)

        def late_send(dd, target):
            send(late_strip(dd, s), late_sem.at[dd, s], (s, target))

        def late_x():
            for i in range(1, xs):
                late_send(d, mine(i))

        def late_y():
            for i in range(xs):
                if i:
                    arrived(late_strip(mine(i), s), late_sem.at[mine(i), s])
                for j in range(1, ys):
                    late_send(mine(i), index(along_y(j), x, core))

        def late_z():
            for i in range(chips):
                dd = mine(i)
                if i >= xs:
                    arrived(late_strip(dd, s), late_sem.at[dd, s])
                send_if(s + 1 < sp, late_strip(dd, s), late_sem.at[dd, s], lax.rem(s + 1, sp))
                send_if(s > 0, late_strip(dd, s), late_sem.at[dd, s], lax.rem(s + sp - 1, sp))
                late_send(dd, sibling)

        def late_forward(k):
            source, target, onward = z_link(k)
            for i in range(chips):
                region, sem = late_strip(mine(i), source), late_sem.at[mine(i), source]

                @pl.when(onward)
                def _():
                    arrived(region, sem)

                send_if(onward, region, sem, target)
                send_if(onward, region, sem, s, sibling)

        def late_last(k):
            source, _, onward = z_link(k)
            ended = jnp.logical_not(onward)
            for i in range(chips):
                region, sem = late_strip(mine(i), source), late_sem.at[mine(i), source]

                @pl.when(ended)
                def _():
                    arrived(region, sem)

                send_if(ended, region, sem, s, sibling)

        def gated_rows(part):
            for copy in loads[part]:
                copy.wait()

            def body(j, carry):
                cs = pl.ds(pl.multiple_of(part * in_cols + j * LANES, LANES), LANES)
                value = v_in[:, cs].astype(F32)
                gate = g_in[:, cs].astype(F32)
                gated[pl.ds(pad, tok), cs] = (value * half_sigmoid(gate)).astype(BF16).astype(F32)
                return carry

            lax.fori_loop(0, in_cols // LANES, body, 0)

        def taps_up():
            for copy in small:
                copy.wait()
            taps_f[...] = taps_in[...].astype(F32)

        def halo_rows():
            @pl.when(s == 0)
            def _():
                gated[pl.ds(0, pad), :] = jnp.zeros((pad, width), F32)

            @pl.when(s > 0)
            def _():
                for copy in halo:
                    copy.wait_recv()

                def body(j, carry):
                    cs = pl.ds(pl.multiple_of(j * LANES, LANES), LANES)
                    value = halo_v[:, cs].astype(F32)
                    gate = halo_g[:, cs].astype(F32)
                    gated[pl.ds(0, pad), cs] = (value * half_sigmoid(gate)).astype(BF16).astype(F32)
                    return carry

                lax.fori_loop(0, blocks, body, 0)

        def mix(row_starts, lo, hi):
            def body(j, carry):
                cs = pl.ds(pl.multiple_of(j * LANES, LANES), LANES)
                for start in row_starts:
                    seen = gated[pl.ds(start, row_chunk + pad), cs]
                    total = None
                    for r in range(8):
                        inner = None
                        length = row_chunk + (8 if r else 0)
                        for q in range(0, pad // 8 + 1):
                            tap = 8 * q + r - lead
                            if 0 <= tap < taps:
                                term = seen[8 * q:8 * q + length] * taps_f[pl.ds(tap, 1), cs]
                                inner = term if inner is None else inner + term
                        if inner is None:
                            continue
                        if r:
                            inner = pltpu.roll(inner, length - r, 0)[:row_chunk]
                        total = inner if total is None else total + inner
                    conv[pl.ds(start, row_chunk), cs] = total.astype(BF16).astype(F32)
                return carry

            lax.fori_loop(lo, hi, body, 0)

        def normalise(low, high):
            step = math.gcd(32, row_chunk)

            def body(i, carry):
                rs = pl.ds(pl.multiple_of(i * step, step), step)
                wide = conv[rs, :]
                mean = jnp.sum(wide, axis=1, keepdims=True) * (1.0 / width)
                centered = wide - mean
                variance = jnp.sum(centered * centered, axis=1, keepdims=True) * (1.0 / width)
                scale = lax.rsqrt(variance + EPSILON)
                normed = centered * scale * gain[...] + shift[...]
                act[rs, :] = (normed * half_sigmoid(normed)).astype(BF16)
                return carry

            lax.fori_loop(low // step, high // step, body, 0)

        def product(dd, part):
            ks = pl.ds(pl.multiple_of(dd * rows, rows), rows)
            ns = pl.ds(pl.multiple_of(part * part_cols, part_cols), part_cols)
            return ns, jnp.dot(act[:, ks], wall[ks, ns], preferred_element_type=F32)

        def sibling_strip(dd, part):
            for half in range(2):
                arrived(strip(half, dd, part), recv_sem.at[half, dd, part])
            if late_rows:
                arrived(late_strip(dd, part), late_sem.at[dd, part])

        def mm_own(c):
            part = part_of[c]
            sibling_strip(sibling, part)
            if streamed:
                ns, first = product(d, part)
                acc[:, ns] = first
                ns, second = product(sibling, part)
                acc[:, ns] += second

        def mm_rest(c):
            part = part_of[c]

            def body(j, carry):
                xx = lax.rem(x + lax.rem(j, xs), xs)
                yy = lax.rem(y + j // xs, ys)
                theirs = index(yy, xx, 1 - core)
                if streamed:
                    ns, first = product(index(yy, xx, core), part)
                    acc[:, ns] += first
                sibling_strip(theirs, part)
                if streamed:
                    ns, second = product(theirs, part)
                    acc[:, ns] += second
                return carry

            lax.fori_loop(1, xs * ys, body, 0)
            if streamed:
                ns = pl.ds(pl.multiple_of(part * part_cols, part_cols), part_cols)
                out_v[0, :, ns] = acc[:, ns].astype(BF16)

        early = [start for start in range(0, tok, row_chunk) if start >= pad]
        late = [start for start in range(0, tok, row_chunk) if start < pad]

        edges = [blocks * i // 4 for i in range(5)]
        z_sends()
        if group > 1:
            send_halo(0)
            for k in range(1, sp):
                z_forward(k)
                z_last(k)
            event_own(0)
        else:
            event_own(0)
            send_halo(0)
        run = {
            "g": (gated_rows, 0, in_parts),
            "t": (lambda c: taps_up(), 0, 1),
            "e": (lambda c: mix(early, edges[c], edges[c + 1]), 0, 4),
            "h": (lambda c: halo_rows(), 0, 1),
            "l": (lambda c: mix(late, edges[c], edges[c + 1]), 0, 4),
            "n": (lambda c: normalise(*((late[-1] + row_chunk, tok), (0, late[-1] + row_chunk))[c]), 0, 2),
            "z": (z_forward, 1, sp if group == 1 else 0),
            "o": (event_own, 1, parts),
            "f": (event_first, 0, parts),
            "s": (event_second, 0, parts),
            "a": (lambda c: send_halo(1), 0, 1),
            "x": (lambda c: late_x(), 0, 1 if late_rows else 0),
            "y": (lambda c: late_y(), 0, 1 if late_rows else 0),
            "v": (lambda c: late_z(), 0, 1 if late_rows else 0),
            "w": (late_forward, 1, sp if late_rows else 0),
            "u": (late_last, 1, sp if late_rows else 0),
            "m": (mm_own, 0, parts),
            "r": (mm_rest, 0, parts),
        }
        order = list(ORDER)
        for c in range(max(sp, parts)):
            order += [kind + str(c) for kind in "zowufsmr" if kind + str(c) not in order]
        for name in order:
            act_on, low, high = run[name[0]]
            if low <= int(name[1:]) < high:
                act_on(int(name[1:]))

        if not streamed:
            k_step = 2 * LANES
            n_step = 4 * LANES

            def body(i, carry):
                ns = pl.ds(pl.multiple_of(i * n_step, n_step), n_step)
                acc[:, ns] = jnp.zeros((tok, n_step), F32)

                def inner(k, carry):
                    ks = pl.ds(pl.multiple_of(k * k_step, k_step), k_step)
                    acc[:, ns] += jnp.dot(act[:, ks], wall[ks, ns], preferred_element_type=F32)
                    return carry

                lax.fori_loop(0, width // k_step, inner, 0)
                out_v[0, :, ns] = acc[:, ns].astype(BF16)
                return carry

            lax.fori_loop(0, width // n_step, body, 0)

        for copy in sent:
            copy.wait_send()

        for wanted, copy in guarded:
            @pl.when(wanted)
            def _():
                copy.wait_send()

        @pl.when(s < sp - 1)
        def _():
            for copy in halo:
                copy.wait_send()

    per_half = [(xs, ys), (ys, xs)]
    sends = xs - 1 + xs * (ys - 1) + chips if late_rows else 0
    for one, two in per_half:
        sends += parts * (one + two - 1) + parts * (one - 1) * two + parts * one * (two - 1)
    scratch = [
        pltpu.VMEM((tok, width), BF16),
        pltpu.VMEM((tok, width), BF16),
        pltpu.VMEM((pad, width), BF16),
        pltpu.VMEM((pad, width), BF16),
        pltpu.VMEM((taps, width), BF16),
        pltpu.VMEM((taps, width), F32),
        pltpu.VMEM((1, width), F32),
        pltpu.VMEM((1, width), F32),
        pltpu.VMEM((pad + tok, width), F32),
        pltpu.VMEM((tok, width), F32),
        pltpu.VMEM((tok, width), BF16),
        pltpu.VMEM((tok, width), F32),
        pltpu.VMEM((dp * rows, sp * cols), BF16),
        pltpu.SemaphoreType.DMA((4 + 2 * in_parts,)),
        pltpu.SemaphoreType.DMA((2,)),
        pltpu.SemaphoreType.DMA((2,)),
        pltpu.SemaphoreType.DMA((sends,)),
        pltpu.SemaphoreType.DMA((2 * (sp + 1) + chips * (3 * sp - 1),)),
        pltpu.SemaphoreType.DMA((2, sp)),
        pltpu.SemaphoreType.DMA((2, dp, parts)),
        pltpu.SemaphoreType.DMA((dp, sp) if late_rows else (1, 1)),
    ]
    return kernel, scratch


def solution(mesh):
    sp, dp = mesh.shape["sp"], mesh.shape["dp"]
    chips = dp // 2
    xs = max(i for i in range(1, math.isqrt(chips) + 1) if chips % i == 0)
    ys = chips // xs
    parts = math.gcd(sp, max(1, 32 // dp))

    def per_device(value_half, gate_half, conv_taps, norm_gain, norm_shift, out_weight):
        _, tok, width = value_half.shape
        taps = conv_taps.shape[0]
        rows, cols = out_weight.shape
        pad = -(-(taps - 1) // 16) * 16
        kernel, scratch = make_kernel(sp, dp, xs, ys, parts, tok, width, taps, rows, cols, pad)
        return pl.pallas_call(
            kernel,
            out_shape=pltpu.VMEM(value_half.shape, BF16),
            in_specs=[pl.BlockSpec(memory_space=pltpu.HBM)] * 6,
            out_specs=pl.BlockSpec(memory_space=pltpu.VMEM),
            scratch_shapes=scratch,
            compiler_params=pltpu.CompilerParams(
                collective_id=0, has_side_effects=True, vmem_limit_bytes=VMEM_LIMIT),
        )(value_half, gate_half, conv_taps, norm_gain[None], norm_shift[None], out_weight)

    placed = (P("dp", "sp", None), P("dp", "sp", None), P(), P(), P(), P("dp", "sp"))
    return jax.shard_map(
        per_device, mesh=mesh, in_specs=placed, out_specs=P("dp", "sp", None), check_vma=False
    )
```

```python
import math
from functools import partial

import jax
import jax.numpy as jnp
from jax import lax
from jax.experimental import pallas as pl
from jax.experimental.pallas import tpu as pltpu
from jax.sharding import PartitionSpec as P

EPSILON = 1e-06
MESH = pl.DeviceIdType.MESH
F32 = jnp.float32
BF16 = jnp.bfloat16
LANES = 128
VMEM_LIMIT = 62 * 1024 * 1024
ORDER = (
    "y0", "i0", "x0", "i1", "o01", "o00", "g3", "b0", "y1", "g2", "t0", "z10", "o10", "z20", "v0", "g1",
    "e1", "z11", "z21", "f01", "o11", "g0", "a0", "e3", "f00", "o20", "e2", "o21", "z30", "z31", "w10", "v3",
    "e0", "f11", "v1", "h0", "s00", "v2", "s03", "n0", "f20", "l2", "w20", "o30", "s11", "l1", "l0", "s20",
    "o31", "w21", "w11", "u10", "w30", "s10", "l3", "w12", "f21", "w22", "f10", "w13", "u20", "n1", "w23", "u12",
    "m00", "s30", "m10", "s02", "s21", "m20", "m02", "w31", "u11", "s01", "u30", "f30", "f31", "w32", "u21", "u22",
    "u13", "m03", "m30", "s13", "w33", "m22", "m12", "s12", "m01", "s31", "m21", "u31", "u23", "s22", "s23", "m13",
    "m11", "s32", "u32", "u33", "s33", "m23", "m31", "m32", "m33",
)


def half_sigmoid(x):
    return 0.5 * jnp.tanh(0.5 * x) + 0.5


def nearest(me, count, k):
    place = jnp.int32(0)
    for here in range(count):
        there = sorted(range(count), key=lambda j: (abs(j - here), j))[k]
        place = place + jnp.where(me == here, there, 0).astype(jnp.int32)
    return place


def make_kernel(sp, dp, xs, ys, parts, tok, width, taps, rows, cols, pad):
    group = sp // parts
    part_cols = group * cols
    late_rows = rows * 3 // 16 // 8 * 8 if group == 1 else 0
    first_rows = (rows - late_rows - late_rows // 4) // 2 // 8 * 8
    half_rows = (first_rows, rows - late_rows - first_rows)
    half_start = (0, first_rows)
    chips = xs * ys
    blocks = width // LANES
    row_chunk = 128 if tok % 128 == 0 else tok
    lead = pad - (taps - 1)
    in_parts = 4 if blocks % 4 == 0 else 1
    in_cols = width // in_parts
    streamed = rows % LANES == 0

    def kernel(v_hbm, g_hbm, taps_hbm, gain_hbm, shift_hbm, w_hbm, out_v,
               v_in, g_in, v_tail, g_tail, tail, halo, taps_in, taps_f, gain, shift, gated, conv, act, acc, wall,
               in_sem, halo_sem, send_sem, z_send, z_sem, recv_sem, late_sem):
        s = lax.axis_index("sp")
        d = lax.axis_index("dp")
        core = lax.rem(d, 2)
        x = lax.rem(d // 2, xs)
        y = d // (2 * xs)

        def index(yy, xx, cc):
            return (yy * xs + xx) * 2 + cc

        sibling = index(y, x, 1 - core)

        def along_x(step):
            return lax.rem(x + step, xs)

        def along_y(step):
            return lax.rem(y + step, ys)

        own = wall.at[pl.ds(pl.multiple_of(d * rows, rows), rows), pl.ds(pl.multiple_of(s * cols, cols), cols)]
        w_copy = pltpu.make_async_copy(w_hbm, own, in_sem.at[0])
        w_copy.start()
        tails = [
            pltpu.make_async_copy(src.at[0, pl.ds(tok - pad, pad), :], dst, in_sem.at[4 + 2 * in_parts + i])
            for i, (src, dst) in enumerate(((v_hbm, v_tail), (g_hbm, g_tail)))
        ]
        for copy in tails:
            copy.start()
        loads = []
        for part in range(in_parts):
            sl = pl.ds(part * in_cols, in_cols)
            pair = (
                pltpu.make_async_copy(v_hbm.at[0, :, sl], v_in.at[:, sl], in_sem.at[4 + 2 * part]),
                pltpu.make_async_copy(g_hbm.at[0, :, sl], g_in.at[:, sl], in_sem.at[5 + 2 * part]),
            )
            loads.append(pair)
            for copy in pair:
                copy.start()
        small = [
            pltpu.make_async_copy(taps_hbm, taps_in, in_sem.at[1]),
            pltpu.make_async_copy(gain_hbm, gain, in_sem.at[2]),
            pltpu.make_async_copy(shift_hbm, shift, in_sem.at[3]),
        ]
        for copy in small:
            copy.start()

        barrier = pltpu.get_barrier_semaphore()
        friends = [(s, sibling)]
        friends += [(s, index(y, along_x(i), core)) for i in range(1, xs)]
        friends += [(s, index(along_y(i), x, core)) for i in range(1, ys)]
        for friend in friends:
            pl.semaphore_signal(barrier, inc=1, device_id=friend, device_id_type=MESH)
        above, below = s + 1 < sp, s > 0

        @pl.when(above)
        def _():
            pl.semaphore_signal(barrier, inc=1, device_id=(lax.rem(s + 1, sp), d), device_id_type=MESH)

        @pl.when(below)
        def _():
            pl.semaphore_signal(barrier, inc=1, device_id=(lax.rem(s + sp - 1, sp), d), device_id_type=MESH)

        pl.semaphore_wait(barrier, len(friends) + above.astype(jnp.int32) + below.astype(jnp.int32))
        w_copy.wait()

        sent = []

        def send(region, sem, target):
            copy = pltpu.make_async_remote_copy(
                src_ref=region, dst_ref=region, send_sem=send_sem.at[len(sent)], recv_sem=sem,
                device_id=target, device_id_type=MESH)
            copy.start()
            sent.append(copy)

        def arrived(region, sem):
            pltpu.make_async_remote_copy(
                src_ref=region, dst_ref=region, send_sem=send_sem.at[0], recv_sem=sem,
                device_id=(s, sibling), device_id_type=MESH).wait_recv()

        def rows_at(dd, half):
            return pl.ds(pl.multiple_of(dd * rows + half_start[half], 8), half_rows[half])

        def block(half, who):
            return wall.at[rows_at(d, half), pl.ds(pl.multiple_of(who * cols, cols), cols)]

        def strip(half, dd, part):
            return wall.at[rows_at(dd, half), pl.ds(pl.multiple_of(part * part_cols, part_cols), part_cols)]

        halo_copy = pltpu.make_async_remote_copy(
            src_ref=tail, dst_ref=halo, send_sem=halo_sem.at[0], recv_sem=halo_sem.at[1],
            device_id=(lax.rem(s + 1, sp), d), device_id_type=MESH)

        def send_halo():
            @pl.when(s < sp - 1)
            def _():
                halo_copy.start()

        guarded = []

        def send_if(wanted, region, sem, target, column=None):
            copy = pltpu.make_async_remote_copy(
                src_ref=region, dst_ref=region, send_sem=z_send.at[len(guarded)], recv_sem=sem,
                device_id=(target, d if column is None else column), device_id_type=MESH)

            @pl.when(wanted)
            def _():
                copy.start()

            guarded.append((wanted, copy))

        def z_sends(half):
            send_if(s + 1 < sp, block(half, s), z_sem.at[half, s], lax.rem(s + 1, sp))
            send_if(s > 0, block(half, s), z_sem.at[half, s], lax.rem(s + sp - 1, sp))

        def z_link(k):
            source = nearest(s, sp, k)
            target = jnp.where(source < s, s + 1, s - 1)
            onward = jnp.logical_and(target >= 0, target < sp)
            return source, lax.rem(target + sp, sp), onward

        def z_forward(k, half):
            source, target, onward = z_link(k)

            @pl.when(onward)
            def _():
                arrived(block(half, source), z_sem.at[half, source])

            send_if(onward, block(half, source), z_sem.at[half, source], target)

        def z_last(k, half):
            source, _, onward = z_link(k)

            @pl.when(jnp.logical_not(onward))
            def _():
                arrived(block(half, source), z_sem.at[half, source])

        my_part = s // group
        part_of = [nearest(my_part, parts, k) for k in range(parts)]

        def firsts(half):
            if half == 0:
                return [index(y, along_x(i), core) for i in range(1, xs)]
            return [index(along_y(i), x, core) for i in range(1, ys)]

        def event_own(c, half):
            part = part_of[c]
            if group == 1 and c > 0:
                z_last(c, half)
            for target in firsts(half) + firsts(1 - half):
                send(strip(half, d, part), recv_sem.at[half, d, part], (s, target))
            send(strip(half, d, part), recv_sem.at[half, d, part], (s, sibling))

        def event_first(c, half):
            part = part_of[c]
            for dd in firsts(half):
                region, sem = strip(half, dd, part), recv_sem.at[half, dd, part]
                arrived(region, sem)
                for target in firsts(1 - half):
                    send(region, sem, (s, target))
                send(region, sem, (s, sibling))

        seconds = []
        for one in range(max(xs, ys)):
            for two in range(1, max(xs, ys)):
                for half in range(2):
                    fx, fy = (one, two) if half == 0 else (two, one)
                    if fx < xs and fy < ys:
                        seconds.append((half, fx, fy))

        def event_second(c, q):
            part = part_of[c]
            half, fx, fy = seconds[q]
            dd = index(along_y(fy), along_x(fx), core)
            region, sem = strip(half, dd, part), recv_sem.at[half, dd, part]
            arrived(region, sem)
            send(region, sem, (s, sibling))

        def late_strip(dd, who):
            return wall.at[pl.ds(pl.multiple_of(dd * rows + rows - late_rows, 8), late_rows),
                           pl.ds(pl.multiple_of(who * cols, cols), cols)]

        def mine(i):
            return index(along_y(i // xs), along_x(i % xs), core)

        def late_send(dd, target):
            send(late_strip(dd, s), late_sem.at[dd, s], (s, target))

        def late_x():
            for i in range(1, xs):
                late_send(d, mine(i))

        def late_y(c):
            for i in range(1, xs) if c else (0,):
                if i:
                    arrived(late_strip(mine(i), s), late_sem.at[mine(i), s])
                for j in range(1, ys):
                    late_send(mine(i), index(along_y(j), x, core))

        def late_z(i):
            dd = mine(i)
            if i >= xs:
                arrived(late_strip(dd, s), late_sem.at[dd, s])
            send_if(s + 1 < sp, late_strip(dd, s), late_sem.at[dd, s], lax.rem(s + 1, sp))
            send_if(s > 0, late_strip(dd, s), late_sem.at[dd, s], lax.rem(s + sp - 1, sp))
            late_send(dd, sibling)

        def late_forward(k, i):
            source, target, onward = z_link(k)
            region, sem = late_strip(mine(i), source), late_sem.at[mine(i), source]

            @pl.when(onward)
            def _():
                arrived(region, sem)

            send_if(onward, region, sem, target)
            send_if(onward, region, sem, s, sibling)

        def late_last(k, i):
            source, _, onward = z_link(k)
            ended = jnp.logical_not(onward)
            region, sem = late_strip(mine(i), source), late_sem.at[mine(i), source]

            @pl.when(ended)
            def _():
                arrived(region, sem)

            send_if(ended, region, sem, s, sibling)

        def gate_tail():
            for copy in tails:
                copy.wait()

            def body(j, carry):
                cs = pl.ds(pl.multiple_of(j * LANES, LANES), LANES)
                tail[:, cs] = (v_tail[:, cs].astype(F32) * half_sigmoid(g_tail[:, cs].astype(F32))).astype(BF16)
                return carry

            lax.fori_loop(0, blocks, body, 0)

        def gated_rows(part):
            for copy in loads[part]:
                copy.wait()

            def body(j, carry):
                cs = pl.ds(pl.multiple_of(part * in_cols + j * LANES, LANES), LANES)
                value = v_in[:, cs].astype(F32)
                gate = g_in[:, cs].astype(F32)
                gated[pl.ds(pad, tok), cs] = (value * half_sigmoid(gate)).astype(BF16).astype(F32)
                return carry

            lax.fori_loop(0, in_cols // LANES, body, 0)

        def taps_up():
            for copy in small:
                copy.wait()
            taps_f[...] = taps_in[...].astype(F32)

        def halo_rows():
            @pl.when(s == 0)
            def _():
                gated[pl.ds(0, pad), :] = jnp.zeros((pad, width), F32)

            @pl.when(s > 0)
            def _():
                halo_copy.wait_recv()

                def body(j, carry):
                    cs = pl.ds(pl.multiple_of(j * LANES, LANES), LANES)
                    gated[pl.ds(0, pad), cs] = halo[:, cs].astype(F32)
                    return carry

                lax.fori_loop(0, blocks, body, 0)

        def mix(row_starts, lo, hi):
            def body(j, carry):
                cs = pl.ds(pl.multiple_of(j * LANES, LANES), LANES)
                for start in row_starts:
                    seen = gated[pl.ds(start, row_chunk + pad), cs]
                    total = None
                    for r in range(8):
                        inner = None
                        length = row_chunk + (8 if r else 0)
                        for q in range(0, pad // 8 + 1):
                            tap = 8 * q + r - lead
                            if 0 <= tap < taps:
                                term = seen[8 * q:8 * q + length] * taps_f[pl.ds(tap, 1), cs]
                                inner = term if inner is None else inner + term
                        if inner is None:
                            continue
                        if r:
                            inner = pltpu.roll(inner, length - r, 0)[:row_chunk]
                        total = inner if total is None else total + inner
                    conv[pl.ds(start, row_chunk), cs] = total.astype(BF16).astype(F32)
                return carry

            lax.fori_loop(lo, hi, body, 0)

        def normalise(low, high):
            step = math.gcd(64, row_chunk)

            def body(i, carry):
                rs = pl.ds(pl.multiple_of(i * step, step), step)
                columns = [slice(j * LANES, (j + 1) * LANES) for j in range(blocks)]
                total = conv[rs, columns[0]]
                for cs in columns[1:]:
                    total = total + conv[rs, cs]
                mean = jnp.sum(total, axis=1, keepdims=True) * (1.0 / width)
                mean = jnp.broadcast_to(mean, (step, LANES))
                total = jnp.zeros((step, LANES), F32)
                for cs in columns:
                    centered = conv[rs, cs] - mean
                    total = total + centered * centered
                variance = jnp.sum(total, axis=1, keepdims=True) * (1.0 / width)
                scale = jnp.broadcast_to(lax.rsqrt(variance + EPSILON), (step, LANES))
                for cs in columns:
                    half = (conv[rs, cs] - mean) * scale * (0.5 * gain[:, cs]) + 0.5 * shift[:, cs]
                    act[rs, cs] = (half * jnp.tanh(half) + half).astype(BF16)
                return carry

            lax.fori_loop(low // step, high // step, body, 0)

        def sibling_strip(dd, part):
            for half in range(2):
                arrived(strip(half, dd, part), recv_sem.at[half, dd, part])
            if late_rows:
                arrived(late_strip(dd, part), late_sem.at[dd, part])

        multiplied = [0] * parts

        def multiply(c, i):
            part = part_of[c]
            xx, yy = along_x(i % xs), along_y(i // xs)
            sibling_strip(index(yy, xx, 1 - core), part)
            if not streamed:
                return
            ks = pl.ds(pl.multiple_of(index(yy, xx, 0) * rows, 2 * rows), 2 * rows)
            ns = pl.ds(pl.multiple_of(part * part_cols, part_cols), part_cols)
            term = jnp.dot(act[:, ks], wall[ks, ns], preferred_element_type=F32)
            multiplied[c] += 1
            if multiplied[c] == 1:
                acc[:, ns] = term
            elif multiplied[c] < chips:
                acc[:, ns] += term
            else:
                out_v[0, :, ns] = (acc[:, ns] + term).astype(BF16)

        early = [start for start in range(0, tok, row_chunk) if start >= pad]
        late = [start for start in range(0, tok, row_chunk) if start < pad]

        edges = [blocks * i // 4 for i in range(5)]
        small_step = {
            "g": (gated_rows, in_parts),
            "e": (lambda c: mix(early, edges[c], edges[c + 1]), 4),
            "l": (lambda c: mix(late, edges[c], edges[c + 1]), 4),
            "n": (lambda c: normalise(*((late[-1] + row_chunk, tok), (0, late[-1] + row_chunk))[c]), 2),
        }
        run = {
            "t0": taps_up,
            "b0": gate_tail,
            "a0": send_halo,
            "h0": halo_rows,
        }
        for kind, (act_on, count) in small_step.items():
            for c in range(count):
                run[f"{kind}{c}"] = partial(act_on, c)
        for half in range(2):
            run[f"i{half}"] = partial(z_sends, half)
            if group == 1:
                for k in range(1, sp):
                    run[f"z{k}{half}"] = partial(z_forward, k, half)
        for c in range(parts):
            for half in range(2):
                run[f"o{c}{half}"] = partial(event_own, c, half)
                run[f"f{c}{half}"] = partial(event_first, c, half)
            for q in range(len(seconds)):
                run[f"s{c}{q}"] = partial(event_second, c, q)
            for i in range(chips):
                run[f"m{c}{i}"] = partial(multiply, c, i)
        if late_rows:
            run["x0"] = late_x
            run["y0"] = partial(late_y, 0)
            run["y1"] = partial(late_y, 1)
            for i in range(chips):
                run[f"v{i}"] = partial(late_z, i)
                for k in range(1, sp):
                    run[f"w{k}{i}"] = partial(late_forward, k, i)
                    run[f"u{k}{i}"] = partial(late_last, k, i)

        def z_all():
            for k in range(1, sp):
                for half in range(2):
                    z_forward(k, half)
                for half in range(2):
                    z_last(k, half)

        order = [name for name in ORDER if name in run]
        if len(order) < len(run):
            order = [f"{kind}{c}" for kind, count in (("i", 2), ("b", 1), ("g", in_parts), ("a", 1)) for c in range(count)]
            if group > 1:
                run["Z"] = z_all
                order.append("Z")
            for kinds in ("xy", "zo", "te", "f", "v", "wu", "h", "l", "n", "s", "m"):
                order += sorted((name for name in run if name[0] in kinds), key=lambda name: (name[1:], -ord(name[0])))
        for name in order:
            run[name]()

        if not streamed:
            k_step = 2 * LANES
            n_step = 4 * LANES

            def body(i, carry):
                ns = pl.ds(pl.multiple_of(i * n_step, n_step), n_step)
                acc[:, ns] = jnp.zeros((tok, n_step), F32)

                def inner(k, carry):
                    ks = pl.ds(pl.multiple_of(k * k_step, k_step), k_step)
                    acc[:, ns] += jnp.dot(act[:, ks], wall[ks, ns], preferred_element_type=F32)
                    return carry

                lax.fori_loop(0, width // k_step, inner, 0)
                out_v[0, :, ns] = acc[:, ns].astype(BF16)
                return carry

            lax.fori_loop(0, width // n_step, body, 0)

        for copy in sent:
            copy.wait_send()

        for wanted, copy in guarded:
            @pl.when(wanted)
            def _():
                copy.wait_send()

        @pl.when(s < sp - 1)
        def _():
            halo_copy.wait_send()

    per_half = [(xs, ys), (ys, xs)]
    sends = xs - 1 + xs * (ys - 1) + chips if late_rows else 0
    for one, two in per_half:
        sends += parts * (one + two - 1) + parts * (one - 1) * two + parts * one * (two - 1)
    scratch = [
        pltpu.VMEM((tok, width), BF16),
        pltpu.VMEM((tok, width), BF16),
        pltpu.VMEM((pad, width), BF16),
        pltpu.VMEM((pad, width), BF16),
        pltpu.VMEM((pad, width), BF16),
        pltpu.VMEM((pad, width), BF16),
        pltpu.VMEM((taps, width), BF16),
        pltpu.VMEM((taps, width), F32),
        pltpu.VMEM((1, width), F32),
        pltpu.VMEM((1, width), F32),
        pltpu.VMEM((pad + tok, width), F32),
        pltpu.VMEM((tok, width), F32),
        pltpu.VMEM((tok, width), BF16),
        pltpu.VMEM((tok, width), F32),
        pltpu.VMEM((dp * rows, sp * cols), BF16),
        pltpu.SemaphoreType.DMA((6 + 2 * in_parts,)),
        pltpu.SemaphoreType.DMA((2,)),
        pltpu.SemaphoreType.DMA((sends,)),
        pltpu.SemaphoreType.DMA((2 * (sp + 1) + chips * (3 * sp - 1),)),
        pltpu.SemaphoreType.DMA((2, sp)),
        pltpu.SemaphoreType.DMA((2, dp, parts)),
        pltpu.SemaphoreType.DMA((dp, sp) if late_rows else (1, 1)),
    ]
    return kernel, scratch


def solution(mesh):
    sp, dp = mesh.shape["sp"], mesh.shape["dp"]
    chips = dp // 2
    xs = max(i for i in range(1, math.isqrt(chips) + 1) if chips % i == 0)
    ys = chips // xs
    parts = math.gcd(sp, max(1, 32 // dp))

    def per_device(value_half, gate_half, conv_taps, norm_gain, norm_shift, out_weight):
        _, tok, width = value_half.shape
        taps = conv_taps.shape[0]
        rows, cols = out_weight.shape
        pad = -(-(taps - 1) // 16) * 16
        kernel, scratch = make_kernel(sp, dp, xs, ys, parts, tok, width, taps, rows, cols, pad)
        return pl.pallas_call(
            kernel,
            out_shape=pltpu.VMEM(value_half.shape, BF16),
            in_specs=[pl.BlockSpec(memory_space=pltpu.HBM)] * 6,
            out_specs=pl.BlockSpec(memory_space=pltpu.VMEM),
            scratch_shapes=scratch,
            compiler_params=pltpu.CompilerParams(
                collective_id=0, has_side_effects=True, vmem_limit_bytes=VMEM_LIMIT),
        )(value_half, gate_half, conv_taps, norm_gain[None], norm_shift[None], out_weight)

    placed = (P("dp", "sp", None), P("dp", "sp", None), P(), P(), P(), P("dp", "sp"))
    return jax.shard_map(
        per_device, mesh=mesh, in_specs=placed, out_specs=P("dp", "sp", None), check_vma=False
    )
```

```python
import math
from functools import partial

import jax
import jax.numpy as jnp
from jax import lax
from jax.experimental import pallas as pl
from jax.experimental.pallas import tpu as pltpu
from jax.sharding import PartitionSpec as P

EPSILON = 1e-06
MESH = pl.DeviceIdType.MESH
F32 = jnp.float32
BF16 = jnp.bfloat16
LANES = 128
VMEM_LIMIT = 62 * 1024 * 1024
ORDER = (
    "y0", "i0", "x0", "i1", "o01", "o00", "g3", "b0", "y1", "g2", "t0", "z10", "o10", "z20", "v0", "g1",
    "e1", "z11", "z21", "f01", "o11", "g0", "a0", "e3", "f00", "o20", "e2", "o21", "z30", "z31", "w10", "v3",
    "e0", "f11", "v1", "h0", "s00", "v2", "s03", "n0", "f20", "l2", "w20", "o30", "s11", "l1", "l0", "s20",
    "o31", "w21", "w11", "u10", "w30", "s10", "l3", "w12", "f21", "w22", "f10", "w13", "u20", "n1", "w23", "u12",
    "m00", "s30", "m10", "s02", "s21", "m20", "m02", "w31", "u11", "s01", "u30", "f30", "f31", "w32", "u21", "u22",
    "u13", "m03", "m30", "s13", "w33", "m22", "m12", "s12", "m01", "s31", "m21", "u31", "u23", "s22", "s23", "m13",
    "m11", "s32", "u32", "u33", "s33", "m23", "m31", "m32", "m33",
)


def half_sigmoid(x):
    return 0.5 * jnp.tanh(0.5 * x) + 0.5


def nearest(me, count, k):
    place = jnp.int32(0)
    for here in range(count):
        there = sorted(range(count), key=lambda j: (abs(j - here), j))[k]
        place = place + jnp.where(me == here, there, 0).astype(jnp.int32)
    return place


def make_kernel(sp, dp, xs, ys, parts, tok, width, taps, rows, cols, pad):
    group = sp // parts
    part_cols = group * cols
    late_rows = rows * 3 // 16 // 8 * 8 if group == 1 else 0
    first_rows = (rows - late_rows - late_rows // 4) // 2 // 8 * 8
    half_rows = (first_rows, rows - late_rows - first_rows)
    half_start = (0, first_rows)
    chips = xs * ys
    blocks = width // LANES
    row_chunk = 128 if tok % 128 == 0 else tok
    lead = pad - (taps - 1)
    in_parts = 4 if blocks % 4 == 0 else 1
    in_cols = width // in_parts
    streamed = rows % LANES == 0

    def kernel(v_hbm, g_hbm, taps_hbm, gain_hbm, shift_hbm, w_hbm, out_v,
               v_in, g_in, v_tail, g_tail, tail, halo, taps_in, taps_f, gain, shift, gated, conv, act, acc, wall,
               in_sem, halo_sem, send_sem, z_sem, recv_sem, late_sem, pair_sem):
        s = lax.axis_index("sp")
        d = lax.axis_index("dp")
        core = lax.rem(d, 2)
        x = lax.rem(d // 2, xs)
        y = d // (2 * xs)

        def index(yy, xx, cc):
            return (yy * xs + xx) * 2 + cc

        sibling = index(y, x, 1 - core)

        def along_x(step):
            return lax.rem(x + step, xs)

        def along_y(step):
            return lax.rem(y + step, ys)

        own = wall.at[pl.ds(pl.multiple_of(d * rows, rows), rows), pl.ds(pl.multiple_of(s * cols, cols), cols)]
        w_copy = pltpu.make_async_copy(w_hbm, own, in_sem.at[0])
        w_copy.start()
        tails = [
            pltpu.make_async_copy(src.at[0, pl.ds(tok - pad, pad), :], dst, in_sem.at[4 + i])
            for i, (src, dst) in enumerate(((v_hbm, v_tail), (g_hbm, g_tail)))
        ]
        for copy in tails:
            copy.start()
        loads = []
        for part in range(in_parts):
            sl = pl.ds(part * in_cols, in_cols)
            pair = (
                pltpu.make_async_copy(v_hbm.at[0, :, sl], v_in.at[:, sl], in_sem.at[6 + 2 * part]),
                pltpu.make_async_copy(g_hbm.at[0, :, sl], g_in.at[:, sl], in_sem.at[7 + 2 * part]),
            )
            loads.append(pair)
            for copy in pair:
                copy.start()
        small = [
            pltpu.make_async_copy(taps_hbm, taps_in, in_sem.at[1]),
            pltpu.make_async_copy(gain_hbm, gain, in_sem.at[2]),
            pltpu.make_async_copy(shift_hbm, shift, in_sem.at[3]),
        ]
        for copy in small:
            copy.start()

        barrier = pltpu.get_barrier_semaphore()
        friends = [(s, sibling)]
        friends += [(s, index(y, along_x(i), core)) for i in range(1, xs)]
        friends += [(s, index(along_y(i), x, core)) for i in range(1, ys)]
        for friend in friends:
            pl.semaphore_signal(barrier, inc=1, device_id=friend, device_id_type=MESH)
        above, below = s + 1 < sp, s > 0

        @pl.when(above)
        def _():
            pl.semaphore_signal(barrier, inc=1, device_id=(lax.rem(s + 1, sp), d), device_id_type=MESH)

        @pl.when(below)
        def _():
            pl.semaphore_signal(barrier, inc=1, device_id=(lax.rem(s + sp - 1, sp), d), device_id_type=MESH)

        pl.semaphore_wait(barrier, len(friends) + above.astype(jnp.int32) + below.astype(jnp.int32))
        w_copy.wait()

        sent = [0, 0]

        def send(region, sem, target):
            copy = pltpu.make_async_remote_copy(
                src_ref=region, dst_ref=region, send_sem=send_sem.at[0], recv_sem=sem,
                device_id=target, device_id_type=MESH)
            copy.start()
            sent[0] += region.shape[0] * region.shape[1]

        def arrived(region, sem):
            pltpu.make_async_remote_copy(
                src_ref=region, dst_ref=region, send_sem=send_sem.at[0], recv_sem=sem,
                device_id=(s, sibling), device_id_type=MESH).wait_recv()

        def left(size, sem):
            units = size // LANES
            wide = max(j for j in range(1, blocks + 1) if units % (8 * j) == 0 and units // j <= dp * rows)
            region = wall.at[pl.ds(0, units // wide), pl.ds(0, wide * LANES)]
            pltpu.make_async_remote_copy(
                src_ref=region, dst_ref=region, send_sem=sem, recv_sem=pair_sem.at[0, 0],
                device_id=(s, sibling), device_id_type=MESH).wait_send()

        def rows_at(dd, half):
            return pl.ds(pl.multiple_of(dd * rows + half_start[half], 8), half_rows[half])

        def block(half, who):
            return wall.at[rows_at(d, half), pl.ds(pl.multiple_of(who * cols, cols), cols)]

        def strip(half, dd, part):
            return wall.at[rows_at(dd, half), pl.ds(pl.multiple_of(part * part_cols, part_cols), part_cols)]

        halo_copy = pltpu.make_async_remote_copy(
            src_ref=tail, dst_ref=halo, send_sem=halo_sem.at[0], recv_sem=halo_sem.at[1],
            device_id=(lax.rem(s + 1, sp), d), device_id_type=MESH)

        def send_halo():
            @pl.when(s < sp - 1)
            def _():
                halo_copy.start()

        def send_if(wanted, region, sem, target, column=None):
            copy = pltpu.make_async_remote_copy(
                src_ref=region, dst_ref=region, send_sem=send_sem.at[1 if column is None else 2], recv_sem=sem,
                device_id=(target, d if column is None else column), device_id_type=MESH)

            @pl.when(wanted)
            def _():
                copy.start()

        def z_sends(half):
            send_if(s + 1 < sp, block(half, s), z_sem.at[half, s], lax.rem(s + 1, sp))
            send_if(s > 0, block(half, s), z_sem.at[half, s], lax.rem(s + sp - 1, sp))

        def z_link(k):
            source = nearest(s, sp, k)
            target = jnp.where(source < s, s + 1, s - 1)
            onward = jnp.logical_and(target >= 0, target < sp)
            return source, lax.rem(target + sp, sp), onward

        def z_forward(k, half):
            source, target, onward = z_link(k)

            @pl.when(onward)
            def _():
                arrived(block(half, source), z_sem.at[half, source])

            send_if(onward, block(half, source), z_sem.at[half, source], target)

        def z_last(k, half):
            source, _, onward = z_link(k)

            @pl.when(jnp.logical_not(onward))
            def _():
                arrived(block(half, source), z_sem.at[half, source])

        my_part = s // group
        part_of = [nearest(my_part, parts, k) for k in range(parts)]

        def firsts(half):
            if half == 0:
                return [index(y, along_x(i), core) for i in range(1, xs)]
            return [index(along_y(i), x, core) for i in range(1, ys)]

        def event_own(c, half):
            part = part_of[c]
            if group == 1 and c > 0:
                z_last(c, half)
            for target in firsts(half) + firsts(1 - half):
                send(strip(half, d, part), recv_sem.at[half, d // 2, part], (s, target))
            send(strip(half, d, part), pair_sem.at[d // 2, part], (s, sibling))

        def event_first(c, half):
            part = part_of[c]
            for dd in firsts(half):
                region, sem = strip(half, dd, part), recv_sem.at[half, dd // 2, part]
                arrived(region, sem)
                for target in firsts(1 - half):
                    send(region, sem, (s, target))
                send(region, pair_sem.at[dd // 2, part], (s, sibling))

        seconds = []
        for one in range(max(xs, ys)):
            for two in range(1, max(xs, ys)):
                for half in range(2):
                    fx, fy = (one, two) if half == 0 else (two, one)
                    if fx < xs and fy < ys:
                        seconds.append((half, fx, fy))

        def event_second(c, q):
            part = part_of[c]
            half, fx, fy = seconds[q]
            dd = index(along_y(fy), along_x(fx), core)
            region = strip(half, dd, part)
            arrived(region, recv_sem.at[half, dd // 2, part])
            send(region, pair_sem.at[dd // 2, part], (s, sibling))

        def late_strip(dd, who):
            return wall.at[pl.ds(pl.multiple_of(dd * rows + rows - late_rows, 8), late_rows),
                           pl.ds(pl.multiple_of(who * cols, cols), cols)]

        def mine(i):
            return index(along_y(i // xs), along_x(i % xs), core)

        def late_send(dd, target, sem=None):
            send(late_strip(dd, s), late_sem.at[dd // 2, s] if sem is None else sem, (s, target))

        def late_x():
            for i in range(1, xs):
                late_send(d, mine(i))

        def late_y(c):
            for i in range(1, xs) if c else (0,):
                if i:
                    arrived(late_strip(mine(i), s), late_sem.at[mine(i) // 2, s])
                for j in range(1, ys):
                    late_send(mine(i), index(along_y(j), x, core))

        def late_z(i):
            dd = mine(i)
            if i >= xs:
                arrived(late_strip(dd, s), late_sem.at[dd // 2, s])
            send_if(s + 1 < sp, late_strip(dd, s), late_sem.at[dd // 2, s], lax.rem(s + 1, sp))
            send_if(s > 0, late_strip(dd, s), late_sem.at[dd // 2, s], lax.rem(s + sp - 1, sp))
            late_send(dd, sibling, pair_sem.at[dd // 2, s])

        def late_forward(k, i):
            source, target, onward = z_link(k)
            region, sem = late_strip(mine(i), source), late_sem.at[mine(i) // 2, source]

            @pl.when(onward)
            def _():
                arrived(region, sem)

            send_if(onward, region, sem, target)
            send_if(onward, region, pair_sem.at[mine(i) // 2, source], s, sibling)

        def late_last(k, i):
            source, _, onward = z_link(k)
            ended = jnp.logical_not(onward)
            region, sem = late_strip(mine(i), source), late_sem.at[mine(i) // 2, source]

            @pl.when(ended)
            def _():
                arrived(region, sem)

            send_if(ended, region, pair_sem.at[mine(i) // 2, source], s, sibling)
            sent[1] += region.shape[0] * region.shape[1]

        def gate_tail():
            for copy in tails:
                copy.wait()

            def body(j, carry):
                cs = pl.ds(pl.multiple_of(j * LANES, LANES), LANES)
                tail[:, cs] = (v_tail[:, cs].astype(F32) * half_sigmoid(g_tail[:, cs].astype(F32))).astype(BF16)
                return carry

            lax.fori_loop(0, blocks, body, 0)

        def gated_rows(part):
            for copy in loads[part]:
                copy.wait()

            def body(j, carry):
                cs = pl.ds(pl.multiple_of(part * in_cols + j * LANES, LANES), LANES)
                value = v_in[:, cs].astype(F32)
                gate = g_in[:, cs].astype(F32)
                gated[pl.ds(pad, tok), cs] = (value * half_sigmoid(gate)).astype(BF16).astype(F32)
                return carry

            lax.fori_loop(0, in_cols // LANES, body, 0)

        def taps_up():
            for copy in small:
                copy.wait()
            taps_f[...] = taps_in[...].astype(F32)

        def halo_rows():
            @pl.when(s == 0)
            def _():
                gated[pl.ds(0, pad), :] = jnp.zeros((pad, width), F32)

            @pl.when(s > 0)
            def _():
                halo_copy.wait_recv()

                def body(j, carry):
                    cs = pl.ds(pl.multiple_of(j * LANES, LANES), LANES)
                    gated[pl.ds(0, pad), cs] = halo[:, cs].astype(F32)
                    return carry

                lax.fori_loop(0, blocks, body, 0)

        def mix(row_starts, lo, hi):
            def body(j, carry):
                cs = pl.ds(pl.multiple_of(j * LANES, LANES), LANES)
                for start in row_starts:
                    seen = gated[pl.ds(start, row_chunk + pad), cs]
                    total = None
                    for r in range(8):
                        inner = None
                        length = row_chunk + (8 if r else 0)
                        for q in range(0, pad // 8 + 1):
                            tap = 8 * q + r - lead
                            if 0 <= tap < taps:
                                term = seen[8 * q:8 * q + length] * taps_f[pl.ds(tap, 1), cs]
                                inner = term if inner is None else inner + term
                        if inner is None:
                            continue
                        if r:
                            inner = pltpu.roll(inner, length - r, 0)[:row_chunk]
                        total = inner if total is None else total + inner
                    conv[pl.ds(start, row_chunk), cs] = total.astype(BF16).astype(F32)
                return carry

            lax.fori_loop(lo, hi, body, 0)

        def normalise(low, high):
            step = math.gcd(64, row_chunk)

            def body(i, carry):
                rs = pl.ds(pl.multiple_of(i * step, step), step)
                columns = [slice(j * LANES, (j + 1) * LANES) for j in range(blocks)]
                total = conv[rs, columns[0]]
                for cs in columns[1:]:
                    total = total + conv[rs, cs]
                mean = jnp.sum(total, axis=1, keepdims=True) * (1.0 / width)
                mean = jnp.broadcast_to(mean, (step, LANES))
                total = jnp.zeros((step, LANES), F32)
                for cs in columns:
                    centered = conv[rs, cs] - mean
                    total = total + centered * centered
                variance = jnp.sum(total, axis=1, keepdims=True) * (1.0 / width)
                scale = jnp.broadcast_to(lax.rsqrt(variance + EPSILON), (step, LANES))
                for cs in columns:
                    half = (conv[rs, cs] - mean) * scale * (0.5 * gain[:, cs]) + 0.5 * shift[:, cs]
                    act[rs, cs] = (half * jnp.tanh(half) + half).astype(BF16)
                return carry

            lax.fori_loop(low // step, high // step, body, 0)

        def sibling_strip(dd, part):
            arrived(wall.at[pl.ds(pl.multiple_of(dd * rows, rows), rows),
                            pl.ds(pl.multiple_of(part * part_cols, part_cols), part_cols)], pair_sem.at[dd // 2, part])

        multiplied = [0] * parts

        def multiply(c, i):
            part = part_of[c]
            xx, yy = along_x(i % xs), along_y(i // xs)
            sibling_strip(index(yy, xx, 1 - core), part)
            if not streamed:
                return
            ks = pl.ds(pl.multiple_of(index(yy, xx, 0) * rows, 2 * rows), 2 * rows)
            ns = pl.ds(pl.multiple_of(part * part_cols, part_cols), part_cols)
            term = jnp.dot(act[:, ks], wall[ks, ns], preferred_element_type=F32)
            multiplied[c] += 1
            if multiplied[c] == 1:
                acc[:, ns] = term
            elif multiplied[c] < chips:
                acc[:, ns] += term
            else:
                out_v[0, :, ns] = (acc[:, ns] + term).astype(BF16)

        early = [start for start in range(0, tok, row_chunk) if start >= pad]
        late = [start for start in range(0, tok, row_chunk) if start < pad]

        edges = [blocks * i // 4 for i in range(5)]
        small_step = {
            "g": (gated_rows, in_parts),
            "e": (lambda c: mix(early, edges[c], edges[c + 1]), 4),
            "l": (lambda c: mix(late, edges[c], edges[c + 1]), 4),
            "n": (lambda c: normalise(*((late[-1] + row_chunk, tok), (0, late[-1] + row_chunk))[c]), 2),
        }
        run = {
            "t0": taps_up,
            "b0": gate_tail,
            "a0": send_halo,
            "h0": halo_rows,
        }
        for kind, (act_on, count) in small_step.items():
            for c in range(count):
                run[f"{kind}{c}"] = partial(act_on, c)
        for half in range(2):
            run[f"i{half}"] = partial(z_sends, half)
            if group == 1:
                for k in range(1, sp):
                    run[f"z{k}{half}"] = partial(z_forward, k, half)
        for c in range(parts):
            for half in range(2):
                run[f"o{c}{half}"] = partial(event_own, c, half)
                run[f"f{c}{half}"] = partial(event_first, c, half)
            for q in range(len(seconds)):
                run[f"s{c}{q}"] = partial(event_second, c, q)
            for i in range(chips):
                run[f"m{c}{i}"] = partial(multiply, c, i)
        if late_rows:
            run["x0"] = late_x
            run["y0"] = partial(late_y, 0)
            run["y1"] = partial(late_y, 1)
            for i in range(chips):
                run[f"v{i}"] = partial(late_z, i)
                for k in range(1, sp):
                    run[f"w{k}{i}"] = partial(late_forward, k, i)
                    run[f"u{k}{i}"] = partial(late_last, k, i)

        def z_all():
            for k in range(1, sp):
                for half in range(2):
                    z_forward(k, half)
                for half in range(2):
                    z_last(k, half)

        order = [name for name in ORDER if name in run]
        if len(order) < len(run):
            order = [f"{kind}{c}" for kind, count in (("i", 2), ("b", 1), ("g", in_parts), ("a", 1)) for c in range(count)]
            if group > 1:
                run["Z"] = z_all
                order.append("Z")
            for kinds in ("xy", "zo", "te", "f", "v", "wu", "h", "l", "n", "s", "m"):
                order += sorted((name for name in run if name[0] in kinds), key=lambda name: (name[1:], -ord(name[0])))
        for name in order:
            run[name]()

        if not streamed:
            k_step = 2 * LANES
            n_step = 4 * LANES

            def body(i, carry):
                ns = pl.ds(pl.multiple_of(i * n_step, n_step), n_step)
                acc[:, ns] = jnp.zeros((tok, n_step), F32)

                def inner(k, carry):
                    ks = pl.ds(pl.multiple_of(k * k_step, k_step), k_step)
                    acc[:, ns] += jnp.dot(act[:, ks], wall[ks, ns], preferred_element_type=F32)
                    return carry

                lax.fori_loop(0, width // k_step, inner, 0)
                out_v[0, :, ns] = acc[:, ns].astype(BF16)
                return carry

            lax.fori_loop(0, width // n_step, body, 0)

        left(sent[0], send_sem.at[0])
        if sent[1]:
            left(sent[1], send_sem.at[2])
        ended = jnp.logical_or(s == 0, s == sp - 1)
        for wanted, count in ((ended, 1), (jnp.logical_not(ended), sp + 1)):
            if sp > 1:
                @pl.when(wanted)
                def _():
                    left(count * rows * cols + count * (chips - 1) * late_rows * cols, send_sem.at[1])

        @pl.when(s < sp - 1)
        def _():
            halo_copy.wait_send()

    scratch = [
        pltpu.VMEM((tok, width), BF16),
        pltpu.VMEM((tok, width), BF16),
        pltpu.VMEM((pad, width), BF16),
        pltpu.VMEM((pad, width), BF16),
        pltpu.VMEM((pad, width), BF16),
        pltpu.VMEM((pad, width), BF16),
        pltpu.VMEM((taps, width), BF16),
        pltpu.VMEM((taps, width), F32),
        pltpu.VMEM((1, width), F32),
        pltpu.VMEM((1, width), F32),
        pltpu.VMEM((pad + tok, width), F32),
        pltpu.VMEM((tok, width), F32),
        pltpu.VMEM((tok, width), BF16),
        pltpu.VMEM((tok, width), F32),
        pltpu.VMEM((dp * rows, sp * cols), BF16),
        pltpu.SemaphoreType.DMA((6 + 2 * in_parts,)),
        pltpu.SemaphoreType.DMA((2,)),
        pltpu.SemaphoreType.DMA((3,)),
        pltpu.SemaphoreType.DMA((2, sp)),
        pltpu.SemaphoreType.DMA((2, chips, parts)),
        pltpu.SemaphoreType.DMA((chips, sp) if late_rows else (1, 1)),
        pltpu.SemaphoreType.DMA((chips, parts)),
    ]
    return kernel, scratch


def solution(mesh):
    sp, dp = mesh.shape["sp"], mesh.shape["dp"]
    chips = dp // 2
    xs = max(i for i in range(1, math.isqrt(chips) + 1) if chips % i == 0)
    ys = chips // xs
    parts = math.gcd(sp, max(1, 32 // dp))

    def per_device(value_half, gate_half, conv_taps, norm_gain, norm_shift, out_weight):
        _, tok, width = value_half.shape
        taps = conv_taps.shape[0]
        rows, cols = out_weight.shape
        pad = -(-(taps - 1) // 16) * 16
        kernel, scratch = make_kernel(sp, dp, xs, ys, parts, tok, width, taps, rows, cols, pad)
        return pl.pallas_call(
            kernel,
            out_shape=pltpu.VMEM(value_half.shape, BF16),
            in_specs=[pl.BlockSpec(memory_space=pltpu.HBM)] * 6,
            out_specs=pl.BlockSpec(memory_space=pltpu.VMEM),
            scratch_shapes=scratch,
            compiler_params=pltpu.CompilerParams(
                collective_id=0, has_side_effects=True, vmem_limit_bytes=VMEM_LIMIT),
        )(value_half, gate_half, conv_taps, norm_gain[None], norm_shift[None], out_weight)

    placed = (P("dp", "sp", None), P("dp", "sp", None), P(), P(), P(), P("dp", "sp"))
    return jax.shard_map(
        per_device, mesh=mesh, in_specs=placed, out_specs=P("dp", "sp", None), check_vma=False
    )
```

```python
import math
from functools import partial

import jax
import jax.numpy as jnp
from jax import lax
from jax.experimental import pallas as pl
from jax.experimental.pallas import tpu as pltpu
from jax.sharding import PartitionSpec as P

EPSILON = 1e-06
MESH = pl.DeviceIdType.MESH
F32 = jnp.float32
BF16 = jnp.bfloat16
LANES = 128
VMEM_LIMIT = 62 * 1024 * 1024
ORDER = (
    "o00", "o01", "q0", "q1", "x0", "y0", "i1", "b0", "g1", "i0", "z21", "z11", "g0", "o11", "g3", "t0",
    "e1", "z20", "z10", "f00", "a0", "o10", "e3", "f01", "f11", "z31", "y1", "v2", "g2", "e2", "f10", "z30",
    "v0", "o20", "e0", "n0", "h0", "v1", "w12", "o21", "l2", "s00", "v3", "s02", "l1", "w22", "s10", "w20",
    "o31", "s11", "s01", "l3", "w10", "w11", "s13", "o30", "u12", "w21", "l0", "n1", "u11", "s20", "f20", "f21",
    "w13", "m11", "s03", "w23", "u13", "w30", "f31", "w32", "u22", "m01", "s12", "w31", "m00", "m12", "u20", "m03",
    "f30", "u10", "w33", "s31", "s21", "m02", "s30", "m13", "u21", "u23", "m20", "m22", "s22", "u30", "s23", "m21",
    "u32", "m10", "m30", "u31", "s32", "s33", "m32", "u33", "m23", "m31", "m33",
)


def half_sigmoid(x):
    return 0.5 * jnp.tanh(0.5 * x) + 0.5


def nearest(me, count, k):
    place = jnp.int32(0)
    for here in range(count):
        there = sorted(range(count), key=lambda j: (abs(j - here), j))[k]
        place = place + jnp.where(me == here, there, 0).astype(jnp.int32)
    return place


def make_kernel(sp, dp, xs, ys, parts, tok, width, taps, rows, cols, pad):
    group = sp // parts
    part_cols = group * cols
    late_rows = rows * 3 // 16 // 8 * 8 if group == 1 else 0
    lent = rows // 16 // 8 * 8 if group == 1 else 0
    plane_rows = (rows - lent, rows + lent)
    plane_start = (0, rows - lent)
    half_rows, half_start = [], []
    for whole, start in zip(plane_rows, plane_start):
        one = (whole - late_rows - late_rows // 4) // 2 // 8 * 8
        half_rows.append((one, whole - late_rows - one))
        half_start.append((start + late_rows, start + late_rows + one))
    chips = xs * ys
    blocks = width // LANES
    row_chunk = 128 if tok % 128 == 0 else tok
    lead = pad - (taps - 1)
    in_parts = 4 if blocks % 4 == 0 else 1
    in_cols = width // in_parts
    streamed = rows % LANES == 0

    def kernel(v_hbm, g_hbm, taps_hbm, gain_hbm, shift_hbm, w_hbm, out_v,
               v_in, g_in, v_tail, g_tail, tail, halo, taps_in, taps_f, gain, shift, gated, conv, act, acc, wall,
               in_sem, halo_sem, send_sem, z_sem, recv_sem, late_sem, pair_sem, lent_sem):
        s = lax.axis_index("sp")
        d = lax.axis_index("dp")
        core = lax.rem(d, 2)
        x = lax.rem(d // 2, xs)
        y = d // (2 * xs)

        def index(yy, xx, cc):
            return (yy * xs + xx) * 2 + cc

        sibling = index(y, x, 1 - core)

        def along_x(step):
            return lax.rem(x + step, xs)

        def along_y(step):
            return lax.rem(y + step, ys)

        own = wall.at[pl.ds(pl.multiple_of(d * rows, rows), rows), pl.ds(pl.multiple_of(s * cols, cols), cols)]
        w_copy = pltpu.make_async_copy(w_hbm, own, in_sem.at[0])
        w_copy.start()
        tails = [
            pltpu.make_async_copy(src.at[0, pl.ds(tok - pad, pad), :], dst, in_sem.at[4 + i])
            for i, (src, dst) in enumerate(((v_hbm, v_tail), (g_hbm, g_tail)))
        ]
        for copy in tails:
            copy.start()
        loads = []
        for part in range(in_parts):
            sl = pl.ds(part * in_cols, in_cols)
            pair = (
                pltpu.make_async_copy(v_hbm.at[0, :, sl], v_in.at[:, sl], in_sem.at[6 + 2 * part]),
                pltpu.make_async_copy(g_hbm.at[0, :, sl], g_in.at[:, sl], in_sem.at[7 + 2 * part]),
            )
            loads.append(pair)
            for copy in pair:
                copy.start()
        small = [
            pltpu.make_async_copy(taps_hbm, taps_in, in_sem.at[1]),
            pltpu.make_async_copy(gain_hbm, gain, in_sem.at[2]),
            pltpu.make_async_copy(shift_hbm, shift, in_sem.at[3]),
        ]
        for copy in small:
            copy.start()

        barrier = pltpu.get_barrier_semaphore()
        friends = [(s, sibling)]
        friends += [(s, index(y, along_x(i), core)) for i in range(1, xs)]
        friends += [(s, index(along_y(i), x, core)) for i in range(1, ys)]
        for friend in friends:
            pl.semaphore_signal(barrier, inc=1, device_id=friend, device_id_type=MESH)
        above, below = s + 1 < sp, s > 0

        @pl.when(above)
        def _():
            pl.semaphore_signal(barrier, inc=1, device_id=(lax.rem(s + 1, sp), d), device_id_type=MESH)

        @pl.when(below)
        def _():
            pl.semaphore_signal(barrier, inc=1, device_id=(lax.rem(s + sp - 1, sp), d), device_id_type=MESH)

        pl.semaphore_wait(barrier, len(friends) + above.astype(jnp.int32) + below.astype(jnp.int32))
        w_copy.wait()

        me = d // 2
        sent = [[0, 0], [0, 0]]

        def by_core(act_on):
            def call(*where):
                for cc in range(2):
                    @pl.when(core == cc)
                    def _():
                        act_on(cc, *where)

            return call

        def send(cc, region, sem, target):
            copy = pltpu.make_async_remote_copy(
                src_ref=region, dst_ref=region, send_sem=send_sem.at[0], recv_sem=sem,
                device_id=(s, target), device_id_type=MESH)
            copy.start()
            sent[cc][0] += region.shape[0] * region.shape[1]

        def arrived(region, sem):
            pltpu.make_async_remote_copy(
                src_ref=region, dst_ref=region, send_sem=send_sem.at[0], recv_sem=sem,
                device_id=(s, sibling), device_id_type=MESH).wait_recv()

        def left(size, sem):
            units = size // LANES
            wide = max(j for j in range(1, blocks + 1) if units % (8 * j) == 0 and units // j <= dp * rows)
            region = wall.at[pl.ds(0, units // wide), pl.ds(0, wide * LANES)]
            pltpu.make_async_remote_copy(
                src_ref=region, dst_ref=region, send_sem=sem, recv_sem=pair_sem.at[0, 0],
                device_id=(s, sibling), device_id_type=MESH).wait_send()

        def piece(chip, start, count, part):
            return wall.at[pl.ds(pl.multiple_of(chip * 2 * rows + start, 8), count),
                           pl.ds(pl.multiple_of(part * part_cols, part_cols), part_cols)]

        def block(cc, half, who):
            return wall.at[pl.ds(pl.multiple_of(me * 2 * rows + half_start[cc][half], 8), half_rows[cc][half]),
                           pl.ds(pl.multiple_of(who * cols, cols), cols)]

        def strip(cc, half, chip, part):
            return piece(chip, half_start[cc][half], half_rows[cc][half], part)

        def late_strip(cc, chip, who):
            return piece(chip, plane_start[cc], late_rows, who)

        halo_copy = pltpu.make_async_remote_copy(
            src_ref=tail, dst_ref=halo, send_sem=halo_sem.at[0], recv_sem=halo_sem.at[1],
            device_id=(lax.rem(s + 1, sp), d), device_id_type=MESH)

        def send_halo():
            @pl.when(s < sp - 1)
            def _():
                halo_copy.start()

        def send_if(wanted, region, sem, target, column=None):
            copy = pltpu.make_async_remote_copy(
                src_ref=region, dst_ref=region, send_sem=send_sem.at[1 if column is None else 2], recv_sem=sem,
                device_id=(target, d if column is None else column), device_id_type=MESH)

            @pl.when(wanted)
            def _():
                copy.start()

        def lend(cc):
            if cc == 0:
                send(cc, piece(me, rows - lent, lent, s), lent_sem.at[0], sibling)

        def borrow(cc):
            if cc == 1:
                arrived(piece(me, rows - lent, lent, s), lent_sem.at[0])

        def z_sends(cc, half):
            send_if(s + 1 < sp, block(cc, half, s), z_sem.at[half, s], lax.rem(s + 1, sp))
            send_if(s > 0, block(cc, half, s), z_sem.at[half, s], lax.rem(s + sp - 1, sp))

        def z_link(k):
            source = nearest(s, sp, k)
            target = jnp.where(source < s, s + 1, s - 1)
            onward = jnp.logical_and(target >= 0, target < sp)
            return source, lax.rem(target + sp, sp), onward

        def z_forward(cc, k, half):
            source, target, onward = z_link(k)

            @pl.when(onward)
            def _():
                arrived(block(cc, half, source), z_sem.at[half, source])

            send_if(onward, block(cc, half, source), z_sem.at[half, source], target)

        def z_last(cc, k, half):
            source, _, onward = z_link(k)

            @pl.when(jnp.logical_not(onward))
            def _():
                arrived(block(cc, half, source), z_sem.at[half, source])

        my_part = s // group
        part_of = [nearest(my_part, parts, k) for k in range(parts)]

        def chip_at(fx, fy):
            return along_y(fy) * xs + along_x(fx)

        def firsts(half):
            if half == 0:
                return [chip_at(i, 0) for i in range(1, xs)]
            return [chip_at(0, i) for i in range(1, ys)]

        def event_own(cc, c, half):
            part = part_of[c]
            if group == 1 and c > 0:
                z_last(cc, c, half)
            for chip in firsts(half) + firsts(1 - half):
                send(cc, strip(cc, half, me, part), recv_sem.at[half, me, part], 2 * chip + cc)
            send(cc, strip(cc, half, me, part), pair_sem.at[me, part], sibling)

        def event_first(cc, c, half):
            part = part_of[c]
            for chip in firsts(half):
                region, sem = strip(cc, half, chip, part), recv_sem.at[half, chip, part]
                arrived(region, sem)
                for target in firsts(1 - half):
                    send(cc, region, sem, 2 * target + cc)
                send(cc, region, pair_sem.at[chip, part], sibling)

        seconds = []
        for one in range(max(xs, ys)):
            for two in range(1, max(xs, ys)):
                for half in range(2):
                    fx, fy = (one, two) if half == 0 else (two, one)
                    if fx < xs and fy < ys:
                        seconds.append((half, fx, fy))

        def event_second(cc, c, q):
            half, fx, fy = seconds[q]
            part, chip = part_of[c], chip_at(fx, fy)
            region = strip(cc, half, chip, part)
            arrived(region, recv_sem.at[half, chip, part])
            send(cc, region, pair_sem.at[chip, part], sibling)

        def mine(i):
            return chip_at(i % xs, i // xs)

        def late_x(cc):
            for i in range(1, xs):
                send(cc, late_strip(cc, me, s), late_sem.at[me, s], 2 * mine(i) + cc)

        def late_y(cc, c):
            for i in range(1, xs) if c else (0,):
                region, sem = late_strip(cc, mine(i), s), late_sem.at[mine(i), s]
                if i:
                    arrived(region, sem)
                for j in range(1, ys):
                    send(cc, region, sem, 2 * chip_at(0, j) + cc)

        def late_z(cc, i):
            region, sem = late_strip(cc, mine(i), s), late_sem.at[mine(i), s]
            if i >= xs:
                arrived(region, sem)
            send_if(s + 1 < sp, region, sem, lax.rem(s + 1, sp))
            send_if(s > 0, region, sem, lax.rem(s + sp - 1, sp))
            if cc == 1 and i == 0:
                region = piece(me, rows, late_rows - lent, s)
            send(cc, region, pair_sem.at[mine(i), s], sibling)

        def late_forward(cc, k, i):
            source, target, onward = z_link(k)
            region, sem = late_strip(cc, mine(i), source), late_sem.at[mine(i), source]

            @pl.when(onward)
            def _():
                arrived(region, sem)

            send_if(onward, region, sem, target)
            send_if(onward, region, pair_sem.at[mine(i), source], s, sibling)

        def late_last(cc, k, i):
            source, _, onward = z_link(k)
            ended = jnp.logical_not(onward)
            region, sem = late_strip(cc, mine(i), source), late_sem.at[mine(i), source]

            @pl.when(ended)
            def _():
                arrived(region, sem)

            send_if(ended, region, pair_sem.at[mine(i), source], s, sibling)
            sent[cc][1] += region.shape[0] * region.shape[1]

        def gate_tail():
            for copy in tails:
                copy.wait()

            def body(j, carry):
                cs = pl.ds(pl.multiple_of(j * LANES, LANES), LANES)
                tail[:, cs] = (v_tail[:, cs].astype(F32) * half_sigmoid(g_tail[:, cs].astype(F32))).astype(BF16)
                return carry

            lax.fori_loop(0, blocks, body, 0)

        def gated_rows(part):
            for copy in loads[part]:
                copy.wait()

            def body(j, carry):
                cs = pl.ds(pl.multiple_of(part * in_cols + j * LANES, LANES), LANES)
                value = v_in[:, cs].astype(F32)
                gate = g_in[:, cs].astype(F32)
                gated[pl.ds(pad, tok), cs] = (value * half_sigmoid(gate)).astype(BF16).astype(F32)
                return carry

            lax.fori_loop(0, in_cols // LANES, body, 0)

        def taps_up():
            for copy in small:
                copy.wait()
            taps_f[...] = taps_in[...].astype(F32)

        def halo_rows():
            @pl.when(s == 0)
            def _():
                gated[pl.ds(0, pad), :] = jnp.zeros((pad, width), F32)

            @pl.when(s > 0)
            def _():
                halo_copy.wait_recv()

                def body(j, carry):
                    cs = pl.ds(pl.multiple_of(j * LANES, LANES), LANES)
                    gated[pl.ds(0, pad), cs] = halo[:, cs].astype(F32)
                    return carry

                lax.fori_loop(0, blocks, body, 0)

        def mix(row_starts, lo, hi):
            def body(j, carry):
                cs = pl.ds(pl.multiple_of(j * LANES, LANES), LANES)
                for start in row_starts:
                    seen = gated[pl.ds(start, row_chunk + pad), cs]
                    total = None
                    for r in range(8):
                        inner = None
                        length = row_chunk + (8 if r else 0)
                        for q in range(0, pad // 8 + 1):
                            tap = 8 * q + r - lead
                            if 0 <= tap < taps:
                                term = seen[8 * q:8 * q + length] * taps_f[pl.ds(tap, 1), cs]
                                inner = term if inner is None else inner + term
                        if inner is None:
                            continue
                        if r:
                            inner = pltpu.roll(inner, length - r, 0)[:row_chunk]
                        total = inner if total is None else total + inner
                    conv[pl.ds(start, row_chunk), cs] = total.astype(BF16).astype(F32)
                return carry

            lax.fori_loop(lo, hi, body, 0)

        def normalise(low, high):
            step = math.gcd(64, row_chunk)

            def body(i, carry):
                rs = pl.ds(pl.multiple_of(i * step, step), step)
                columns = [slice(j * LANES, (j + 1) * LANES) for j in range(blocks)]
                total = conv[rs, columns[0]]
                for cs in columns[1:]:
                    total = total + conv[rs, cs]
                mean = jnp.sum(total, axis=1, keepdims=True) * (1.0 / width)
                mean = jnp.broadcast_to(mean, (step, LANES))
                total = jnp.zeros((step, LANES), F32)
                for cs in columns:
                    centered = conv[rs, cs] - mean
                    total = total + centered * centered
                variance = jnp.sum(total, axis=1, keepdims=True) * (1.0 / width)
                scale = jnp.broadcast_to(lax.rsqrt(variance + EPSILON), (step, LANES))
                for cs in columns:
                    half = (conv[rs, cs] - mean) * scale * (0.5 * gain[:, cs]) + 0.5 * shift[:, cs]
                    act[rs, cs] = (half * jnp.tanh(half) + half).astype(BF16)
                return carry

            lax.fori_loop(low // step, high // step, body, 0)

        def sibling_strip(cc, c, i):
            start, count = plane_start[1 - cc], plane_rows[1 - cc]
            if cc == 0 and c == 0 and i == 0:
                start, count = rows, rows
            arrived(piece(mine(i), start, count, part_of[c]), pair_sem.at[mine(i), part_of[c]])

        multiplied = [0] * parts

        def multiply(c, i):
            part = part_of[c]
            by_core(sibling_strip)(c, i)
            if not streamed:
                return
            ks = pl.ds(pl.multiple_of(mine(i) * 2 * rows, 2 * rows), 2 * rows)
            ns = pl.ds(pl.multiple_of(part * part_cols, part_cols), part_cols)
            term = jnp.dot(act[:, ks], wall[ks, ns], preferred_element_type=F32)
            multiplied[c] += 1
            if multiplied[c] == 1:
                acc[:, ns] = term
            elif multiplied[c] < chips:
                acc[:, ns] += term
            else:
                out_v[0, :, ns] = (acc[:, ns] + term).astype(BF16)

        early = [start for start in range(0, tok, row_chunk) if start >= pad]
        late = [start for start in range(0, tok, row_chunk) if start < pad]

        edges = [blocks * i // 4 for i in range(5)]
        small_step = {
            "g": (gated_rows, in_parts),
            "e": (lambda c: mix(early, edges[c], edges[c + 1]), 4),
            "l": (lambda c: mix(late, edges[c], edges[c + 1]), 4),
            "n": (lambda c: normalise(*((late[-1] + row_chunk, tok), (0, late[-1] + row_chunk))[c]), 2),
        }
        run = {
            "t0": taps_up,
            "b0": gate_tail,
            "a0": send_halo,
            "h0": halo_rows,
        }
        for kind, (act_on, count) in small_step.items():
            for c in range(count):
                run[f"{kind}{c}"] = partial(act_on, c)
        for half in range(2):
            run[f"i{half}"] = partial(by_core(z_sends), half)
            if group == 1:
                for k in range(1, sp):
                    run[f"z{k}{half}"] = partial(by_core(z_forward), k, half)
        for c in range(parts):
            for half in range(2):
                run[f"o{c}{half}"] = partial(by_core(event_own), c, half)
                run[f"f{c}{half}"] = partial(by_core(event_first), c, half)
            for q in range(len(seconds)):
                run[f"s{c}{q}"] = partial(by_core(event_second), c, q)
            for i in range(chips):
                run[f"m{c}{i}"] = partial(multiply, c, i)
        if late_rows:
            run["x0"] = by_core(late_x)
            run["q0"] = by_core(lend)
            run["q1"] = by_core(borrow)
            run["y0"] = partial(by_core(late_y), 0)
            run["y1"] = partial(by_core(late_y), 1)
            for i in range(chips):
                run[f"v{i}"] = partial(by_core(late_z), i)
                for k in range(1, sp):
                    run[f"w{k}{i}"] = partial(by_core(late_forward), k, i)
                    run[f"u{k}{i}"] = partial(by_core(late_last), k, i)

        def z_all():
            for k in range(1, sp):
                for half in range(2):
                    by_core(z_forward)(k, half)
                for half in range(2):
                    by_core(z_last)(k, half)

        order = [name for name in ORDER if name in run]
        if len(order) < len(run):
            order = [f"{kind}{c}" for kind, count in (("i", 2), ("b", 1), ("g", in_parts), ("a", 1)) for c in range(count)]
            if group > 1:
                run["Z"] = z_all
                order.append("Z")
            for kinds in ("q", "xy", "zo", "te", "f", "v", "wu", "h", "l", "n", "s", "m"):
                order += sorted((name for name in run if name[0] in kinds), key=lambda name: (name[1:], -ord(name[0])))
        for name in order:
            run[name]()

        if not streamed:
            k_step = 2 * LANES
            n_step = 4 * LANES

            def body(i, carry):
                ns = pl.ds(pl.multiple_of(i * n_step, n_step), n_step)
                acc[:, ns] = jnp.zeros((tok, n_step), F32)

                def inner(k, carry):
                    ks = pl.ds(pl.multiple_of(k * k_step, k_step), k_step)
                    acc[:, ns] += jnp.dot(act[:, ks], wall[ks, ns], preferred_element_type=F32)
                    return carry

                lax.fori_loop(0, width // k_step, inner, 0)
                out_v[0, :, ns] = acc[:, ns].astype(BF16)
                return carry

            lax.fori_loop(0, width // n_step, body, 0)

        ended = jnp.logical_or(s == 0, s == sp - 1)

        def finish(cc):
            left(sent[cc][0], send_sem.at[0])
            if sent[cc][1]:
                left(sent[cc][1], send_sem.at[2])
            for wanted, count in ((ended, 1), (jnp.logical_not(ended), sp + 1)):
                if sp > 1:
                    @pl.when(wanted)
                    def _():
                        left(count * (plane_rows[cc] + (chips - 1) * late_rows) * cols, send_sem.at[1])

        by_core(finish)()

        @pl.when(s < sp - 1)
        def _():
            halo_copy.wait_send()

    scratch = [
        pltpu.VMEM((tok, width), BF16),
        pltpu.VMEM((tok, width), BF16),
        pltpu.VMEM((pad, width), BF16),
        pltpu.VMEM((pad, width), BF16),
        pltpu.VMEM((pad, width), BF16),
        pltpu.VMEM((pad, width), BF16),
        pltpu.VMEM((taps, width), BF16),
        pltpu.VMEM((taps, width), F32),
        pltpu.VMEM((1, width), F32),
        pltpu.VMEM((1, width), F32),
        pltpu.VMEM((pad + tok, width), F32),
        pltpu.VMEM((tok, width), F32),
        pltpu.VMEM((tok, width), BF16),
        pltpu.VMEM((tok, width), F32),
        pltpu.VMEM((dp * rows, sp * cols), BF16),
        pltpu.SemaphoreType.DMA((6 + 2 * in_parts,)),
        pltpu.SemaphoreType.DMA((2,)),
        pltpu.SemaphoreType.DMA((3,)),
        pltpu.SemaphoreType.DMA((2, sp)),
        pltpu.SemaphoreType.DMA((2, chips, parts)),
        pltpu.SemaphoreType.DMA((chips, sp) if late_rows else (1, 1)),
        pltpu.SemaphoreType.DMA((chips, parts)),
        pltpu.SemaphoreType.DMA((1,)),
    ]
    return kernel, scratch


def solution(mesh):
    sp, dp = mesh.shape["sp"], mesh.shape["dp"]
    chips = dp // 2
    xs = max(i for i in range(1, math.isqrt(chips) + 1) if chips % i == 0)
    ys = chips // xs
    parts = math.gcd(sp, max(1, 32 // dp))

    def per_device(value_half, gate_half, conv_taps, norm_gain, norm_shift, out_weight):
        _, tok, width = value_half.shape
        taps = conv_taps.shape[0]
        rows, cols = out_weight.shape
        pad = -(-(taps - 1) // 16) * 16
        kernel, scratch = make_kernel(sp, dp, xs, ys, parts, tok, width, taps, rows, cols, pad)
        return pl.pallas_call(
            kernel,
            out_shape=pltpu.VMEM(value_half.shape, BF16),
            in_specs=[pl.BlockSpec(memory_space=pltpu.HBM)] * 6,
            out_specs=pl.BlockSpec(memory_space=pltpu.VMEM),
            scratch_shapes=scratch,
            compiler_params=pltpu.CompilerParams(
                collective_id=0, has_side_effects=True, vmem_limit_bytes=VMEM_LIMIT),
        )(value_half, gate_half, conv_taps, norm_gain[None], norm_shift[None], out_weight)

    placed = (P("dp", "sp", None), P("dp", "sp", None), P(), P(), P(), P("dp", "sp"))
    return jax.shard_map(
        per_device, mesh=mesh, in_specs=placed, out_specs=P("dp", "sp", None), check_vma=False
    )
```

```python
import math
from functools import partial

import jax
import jax.numpy as jnp
from jax import lax
from jax.experimental import pallas as pl
from jax.experimental.pallas import tpu as pltpu
from jax.sharding import PartitionSpec as P

EPSILON = 1e-06
MESH = pl.DeviceIdType.MESH
F32 = jnp.float32
BF16 = jnp.bfloat16
LANES = 128
VMEM_LIMIT = 62 * 1024 * 1024
ORDER = (
    "i1", "x0", "o00", "b0", "t0", "o01", "y0", "g0", "i0", "g1", "a0", "e1", "e0", "z11", "z21", "o11",
    "z20", "z10", "g2", "v0", "o10", "f01", "y1", "z31", "h0", "o21", "s00", "o20", "l2", "s01", "v1", "g3",
    "l0", "f11", "w20", "z30", "w10", "u10", "v2", "f00", "e3", "o31", "l1", "v3", "e2", "w21", "l3", "w11",
    "u11", "w22", "f20", "o30", "n0", "w23", "w12", "n1", "s11", "s02", "f21", "s03", "m03", "f10", "s20", "s13",
    "w13", "m10", "u13", "m00", "w30", "u21", "u22", "f31", "s21", "w31", "w32", "u12", "f30", "w33", "m22", "u20",
    "s22", "s10", "s31", "m11", "u23", "m01", "m21", "m20", "u30", "s23", "s12", "m02", "m12", "u31", "m30", "m23",
    "u32", "s30", "s33", "m13", "s32", "u33", "m31", "m32", "m33",
)


def half_sigmoid(x):
    return 0.5 * jnp.tanh(0.5 * x) + 0.5


def nearest(me, count, k):
    place = jnp.int32(0)
    for here in range(count):
        there = sorted(range(count), key=lambda j: (abs(j - here), j))[k]
        place = place + jnp.where(me == here, there, 0).astype(jnp.int32)
    return place


def make_kernel(sp, dp, xs, ys, parts, tok, width, taps, rows, cols, pad):
    group = sp // parts
    part_cols = group * cols
    late_rows = [share // 8 * 8 if group == 1 else 0 for share in (rows * 7 // 32, rows * 6 // 32)]
    plane_start = (0, rows)
    half_rows, half_start = [], []
    for core_late, start, lean in zip(late_rows, plane_start, (4, 16)):
        one = (rows - core_late - (lean if core_late else 0)) // 2 // 8 * 8
        half_rows.append((one, rows - core_late - one))
        half_start.append((start + core_late, start + core_late + one))
    chips = xs * ys
    blocks = width // LANES
    row_chunk = 128 if tok % 128 == 0 else tok
    lead = pad - (taps - 1)
    in_parts = 4 if blocks % 4 == 0 else 1
    in_cols = width // in_parts
    streamed = rows % LANES == 0

    def kernel(v_hbm, g_hbm, taps_hbm, gain_hbm, shift_hbm, w_hbm, out_v,
               v_in, g_in, v_tail, g_tail, tail, halo, taps_in, taps_f, gain, shift, gated, conv, act, acc, wall,
               in_sem, halo_sem, send_sem, z_sem, recv_sem, late_sem, pair_sem):
        s = lax.axis_index("sp")
        d = lax.axis_index("dp")
        core = lax.rem(d, 2)
        x = lax.rem(d // 2, xs)
        y = d // (2 * xs)

        def index(yy, xx, cc):
            return (yy * xs + xx) * 2 + cc

        sibling = index(y, x, 1 - core)

        def along_x(step):
            return lax.rem(x + step, xs)

        def along_y(step):
            return lax.rem(y + step, ys)

        own = wall.at[pl.ds(pl.multiple_of(d * rows, rows), rows), pl.ds(pl.multiple_of(s * cols, cols), cols)]
        w_copy = pltpu.make_async_copy(w_hbm, own, in_sem.at[0])
        w_copy.start()
        tails = [
            pltpu.make_async_copy(src.at[0, pl.ds(tok - pad, pad), :], dst, in_sem.at[4 + i])
            for i, (src, dst) in enumerate(((v_hbm, v_tail), (g_hbm, g_tail)))
        ]
        for copy in tails:
            copy.start()
        loads = []
        for part in range(in_parts):
            sl = pl.ds(part * in_cols, in_cols)
            pair = (
                pltpu.make_async_copy(v_hbm.at[0, :, sl], v_in.at[:, sl], in_sem.at[6 + 2 * part]),
                pltpu.make_async_copy(g_hbm.at[0, :, sl], g_in.at[:, sl], in_sem.at[7 + 2 * part]),
            )
            loads.append(pair)
            for copy in pair:
                copy.start()
        small = [
            pltpu.make_async_copy(taps_hbm, taps_in, in_sem.at[1]),
            pltpu.make_async_copy(gain_hbm, gain, in_sem.at[2]),
            pltpu.make_async_copy(shift_hbm, shift, in_sem.at[3]),
        ]
        for copy in small:
            copy.start()

        barrier = pltpu.get_barrier_semaphore()
        friends = [(s, sibling)]
        friends += [(s, index(y, along_x(i), core)) for i in range(1, xs)]
        friends += [(s, index(along_y(i), x, core)) for i in range(1, ys)]
        for friend in friends:
            pl.semaphore_signal(barrier, inc=1, device_id=friend, device_id_type=MESH)
        above, below = s + 1 < sp, s > 0

        @pl.when(above)
        def _():
            pl.semaphore_signal(barrier, inc=1, device_id=(lax.rem(s + 1, sp), d), device_id_type=MESH)

        @pl.when(below)
        def _():
            pl.semaphore_signal(barrier, inc=1, device_id=(lax.rem(s + sp - 1, sp), d), device_id_type=MESH)

        pl.semaphore_wait(barrier, len(friends) + above.astype(jnp.int32) + below.astype(jnp.int32))
        w_copy.wait()

        me = d // 2
        sent = [[0, 0], [0, 0]]

        def by_core(act_on):
            def call(*where):
                for cc in range(2):
                    @pl.when(core == cc)
                    def _():
                        act_on(cc, *where)

            return call

        def send(cc, region, sem, target):
            copy = pltpu.make_async_remote_copy(
                src_ref=region, dst_ref=region, send_sem=send_sem.at[0], recv_sem=sem,
                device_id=(s, target), device_id_type=MESH)
            copy.start()
            sent[cc][0] += region.shape[0] * region.shape[1]

        def arrived(region, sem):
            pltpu.make_async_remote_copy(
                src_ref=region, dst_ref=region, send_sem=send_sem.at[0], recv_sem=sem,
                device_id=(s, sibling), device_id_type=MESH).wait_recv()

        def left(size, sem):
            units = size // LANES
            wide = max(j for j in range(1, blocks + 1) if units % (8 * j) == 0 and units // j <= dp * rows)
            region = wall.at[pl.ds(0, units // wide), pl.ds(0, wide * LANES)]
            pltpu.make_async_remote_copy(
                src_ref=region, dst_ref=region, send_sem=sem, recv_sem=pair_sem.at[0, 0],
                device_id=(s, sibling), device_id_type=MESH).wait_send()

        def piece(chip, start, count, part):
            return wall.at[pl.ds(pl.multiple_of(chip * 2 * rows + start, 8), count),
                           pl.ds(pl.multiple_of(part * part_cols, part_cols), part_cols)]

        def block(cc, half, who):
            return wall.at[pl.ds(pl.multiple_of(me * 2 * rows + half_start[cc][half], 8), half_rows[cc][half]),
                           pl.ds(pl.multiple_of(who * cols, cols), cols)]

        def strip(cc, half, chip, part):
            return piece(chip, half_start[cc][half], half_rows[cc][half], part)

        def late_strip(cc, chip, who):
            return piece(chip, plane_start[cc], late_rows[cc], who)

        halo_copy = pltpu.make_async_remote_copy(
            src_ref=tail, dst_ref=halo, send_sem=halo_sem.at[0], recv_sem=halo_sem.at[1],
            device_id=(lax.rem(s + 1, sp), d), device_id_type=MESH)

        def send_halo():
            @pl.when(s < sp - 1)
            def _():
                halo_copy.start()

        def send_if(wanted, region, sem, target, column=None):
            copy = pltpu.make_async_remote_copy(
                src_ref=region, dst_ref=region, send_sem=send_sem.at[1 if column is None else 2], recv_sem=sem,
                device_id=(target, d if column is None else column), device_id_type=MESH)

            @pl.when(wanted)
            def _():
                copy.start()

        def z_sends(cc, half):
            send_if(s + 1 < sp, block(cc, half, s), z_sem.at[half, s], lax.rem(s + 1, sp))
            send_if(s > 0, block(cc, half, s), z_sem.at[half, s], lax.rem(s + sp - 1, sp))

        def z_link(k):
            source = nearest(s, sp, k)
            target = jnp.where(source < s, s + 1, s - 1)
            onward = jnp.logical_and(target >= 0, target < sp)
            return source, lax.rem(target + sp, sp), onward

        def z_forward(cc, k, half):
            source, target, onward = z_link(k)

            @pl.when(onward)
            def _():
                arrived(block(cc, half, source), z_sem.at[half, source])

            send_if(onward, block(cc, half, source), z_sem.at[half, source], target)

        def z_last(cc, k, half):
            source, _, onward = z_link(k)

            @pl.when(jnp.logical_not(onward))
            def _():
                arrived(block(cc, half, source), z_sem.at[half, source])

        my_part = s // group
        part_of = [nearest(my_part, parts, k) for k in range(parts)]

        def chip_at(fx, fy):
            return along_y(fy) * xs + along_x(fx)

        def firsts(half):
            if half == 0:
                return [chip_at(i, 0) for i in range(1, xs)]
            return [chip_at(0, i) for i in range(1, ys)]

        def event_own(cc, c, half):
            part = part_of[c]
            if group == 1 and c > 0:
                z_last(cc, c, half)
            for chip in firsts(half) + firsts(1 - half):
                send(cc, strip(cc, half, me, part), recv_sem.at[half, me, part], 2 * chip + cc)
            send(cc, strip(cc, half, me, part), pair_sem.at[me, part], sibling)

        def event_first(cc, c, half):
            part = part_of[c]
            for chip in firsts(half):
                region, sem = strip(cc, half, chip, part), recv_sem.at[half, chip, part]
                arrived(region, sem)
                for target in firsts(1 - half):
                    send(cc, region, sem, 2 * target + cc)
                send(cc, region, pair_sem.at[chip, part], sibling)

        seconds = []
        for one in range(max(xs, ys)):
            for two in range(1, max(xs, ys)):
                for half in range(2):
                    fx, fy = (one, two) if half == 0 else (two, one)
                    if fx < xs and fy < ys:
                        seconds.append((half, fx, fy))

        def event_second(cc, c, q):
            half, fx, fy = seconds[q]
            part, chip = part_of[c], chip_at(fx, fy)
            region = strip(cc, half, chip, part)
            arrived(region, recv_sem.at[half, chip, part])
            send(cc, region, pair_sem.at[chip, part], sibling)

        def mine(i):
            return chip_at(i % xs, i // xs)

        def late_x(cc):
            for i in range(1, xs):
                send(cc, late_strip(cc, me, s), late_sem.at[me, s], 2 * mine(i) + cc)

        def late_y(cc, c):
            for i in range(1, xs) if c else (0,):
                region, sem = late_strip(cc, mine(i), s), late_sem.at[mine(i), s]
                if i:
                    arrived(region, sem)
                for j in range(1, ys):
                    send(cc, region, sem, 2 * chip_at(0, j) + cc)

        def late_z(cc, i):
            region, sem = late_strip(cc, mine(i), s), late_sem.at[mine(i), s]
            if i >= xs:
                arrived(region, sem)
            send_if(s + 1 < sp, region, sem, lax.rem(s + 1, sp))
            send_if(s > 0, region, sem, lax.rem(s + sp - 1, sp))
            send(cc, region, pair_sem.at[mine(i), s], sibling)

        def late_forward(cc, k, i):
            source, target, onward = z_link(k)
            region, sem = late_strip(cc, mine(i), source), late_sem.at[mine(i), source]

            @pl.when(onward)
            def _():
                arrived(region, sem)

            send_if(onward, region, sem, target)
            send_if(onward, region, pair_sem.at[mine(i), source], s, sibling)

        def late_last(cc, k, i):
            source, _, onward = z_link(k)
            ended = jnp.logical_not(onward)
            region, sem = late_strip(cc, mine(i), source), late_sem.at[mine(i), source]

            @pl.when(ended)
            def _():
                arrived(region, sem)

            send_if(ended, region, pair_sem.at[mine(i), source], s, sibling)
            sent[cc][1] += region.shape[0] * region.shape[1]

        def gate_tail():
            for copy in tails:
                copy.wait()

            def body(j, carry):
                cs = pl.ds(pl.multiple_of(j * LANES, LANES), LANES)
                tail[:, cs] = (v_tail[:, cs].astype(F32) * half_sigmoid(g_tail[:, cs].astype(F32))).astype(BF16)
                return carry

            lax.fori_loop(0, blocks, body, 0)

        def gated_rows(part):
            for copy in loads[part]:
                copy.wait()

            def body(j, carry):
                cs = pl.ds(pl.multiple_of(part * in_cols + j * LANES, LANES), LANES)
                value = v_in[:, cs].astype(F32)
                gate = g_in[:, cs].astype(F32)
                gated[pl.ds(pad, tok), cs] = (value * half_sigmoid(gate)).astype(BF16).astype(F32)
                return carry

            lax.fori_loop(0, in_cols // LANES, body, 0)

        def taps_up():
            for copy in small:
                copy.wait()
            taps_f[...] = taps_in[...].astype(F32)

        def halo_rows():
            @pl.when(s == 0)
            def _():
                gated[pl.ds(0, pad), :] = jnp.zeros((pad, width), F32)

            @pl.when(s > 0)
            def _():
                halo_copy.wait_recv()

                def body(j, carry):
                    cs = pl.ds(pl.multiple_of(j * LANES, LANES), LANES)
                    gated[pl.ds(0, pad), cs] = halo[:, cs].astype(F32)
                    return carry

                lax.fori_loop(0, blocks, body, 0)

        def mix(row_starts, lo, hi):
            def body(j, carry):
                cs = pl.ds(pl.multiple_of(j * LANES, LANES), LANES)
                for start in row_starts:
                    seen = gated[pl.ds(start, row_chunk + pad), cs]
                    total = None
                    for r in range(8):
                        inner = None
                        length = row_chunk + (8 if r else 0)
                        for q in range(0, pad // 8 + 1):
                            tap = 8 * q + r - lead
                            if 0 <= tap < taps:
                                term = seen[8 * q:8 * q + length] * taps_f[pl.ds(tap, 1), cs]
                                inner = term if inner is None else inner + term
                        if inner is None:
                            continue
                        if r:
                            inner = pltpu.roll(inner, length - r, 0)[:row_chunk]
                        total = inner if total is None else total + inner
                    conv[pl.ds(start, row_chunk), cs] = total.astype(BF16).astype(F32)
                return carry

            lax.fori_loop(lo, hi, body, 0)

        def normalise(low, high):
            step = math.gcd(64, row_chunk)

            def body(i, carry):
                rs = pl.ds(pl.multiple_of(i * step, step), step)
                columns = [slice(j * LANES, (j + 1) * LANES) for j in range(blocks)]
                total = conv[rs, columns[0]]
                for cs in columns[1:]:
                    total = total + conv[rs, cs]
                mean = jnp.sum(total, axis=1, keepdims=True) * (1.0 / width)
                mean = jnp.broadcast_to(mean, (step, LANES))
                total = jnp.zeros((step, LANES), F32)
                for cs in columns:
                    centered = conv[rs, cs] - mean
                    total = total + centered * centered
                variance = jnp.sum(total, axis=1, keepdims=True) * (1.0 / width)
                scale = jnp.broadcast_to(lax.rsqrt(variance + EPSILON), (step, LANES))
                for cs in columns:
                    half = (conv[rs, cs] - mean) * scale * (0.5 * gain[:, cs]) + 0.5 * shift[:, cs]
                    act[rs, cs] = (half * jnp.tanh(half) + half).astype(BF16)
                return carry

            lax.fori_loop(low // step, high // step, body, 0)

        def sibling_strip(cc, c, i):
            arrived(piece(mine(i), plane_start[1 - cc], rows, part_of[c]), pair_sem.at[mine(i), part_of[c]])

        multiplied = [0] * parts

        def multiply(c, i):
            part = part_of[c]
            by_core(sibling_strip)(c, i)
            if not streamed:
                return
            ks = pl.ds(pl.multiple_of(mine(i) * 2 * rows, 2 * rows), 2 * rows)
            ns = pl.ds(pl.multiple_of(part * part_cols, part_cols), part_cols)
            term = jnp.dot(act[:, ks], wall[ks, ns], preferred_element_type=F32)
            multiplied[c] += 1
            if multiplied[c] == 1:
                acc[:, ns] = term
            elif multiplied[c] < chips:
                acc[:, ns] += term
            else:
                out_v[0, :, ns] = (acc[:, ns] + term).astype(BF16)

        early = [start for start in range(0, tok, row_chunk) if start >= pad]
        late = [start for start in range(0, tok, row_chunk) if start < pad]

        edges = [blocks * i // 4 for i in range(5)]
        small_step = {
            "g": (gated_rows, in_parts),
            "e": (lambda c: mix(early, edges[c], edges[c + 1]), 4),
            "l": (lambda c: mix(late, edges[c], edges[c + 1]), 4),
            "n": (lambda c: normalise(*((late[-1] + row_chunk, tok), (0, late[-1] + row_chunk))[c]), 2),
        }
        run = {
            "t0": taps_up,
            "b0": gate_tail,
            "a0": send_halo,
            "h0": halo_rows,
        }
        for kind, (act_on, count) in small_step.items():
            for c in range(count):
                run[f"{kind}{c}"] = partial(act_on, c)
        for half in range(2):
            run[f"i{half}"] = partial(by_core(z_sends), half)
            if group == 1:
                for k in range(1, sp):
                    run[f"z{k}{half}"] = partial(by_core(z_forward), k, half)
        for c in range(parts):
            for half in range(2):
                run[f"o{c}{half}"] = partial(by_core(event_own), c, half)
                run[f"f{c}{half}"] = partial(by_core(event_first), c, half)
            for q in range(len(seconds)):
                run[f"s{c}{q}"] = partial(by_core(event_second), c, q)
            for i in range(chips):
                run[f"m{c}{i}"] = partial(multiply, c, i)
        if group == 1:
            run["x0"] = by_core(late_x)
            run["y0"] = partial(by_core(late_y), 0)
            run["y1"] = partial(by_core(late_y), 1)
            for i in range(chips):
                run[f"v{i}"] = partial(by_core(late_z), i)
                for k in range(1, sp):
                    run[f"w{k}{i}"] = partial(by_core(late_forward), k, i)
                    run[f"u{k}{i}"] = partial(by_core(late_last), k, i)

        def z_all():
            for k in range(1, sp):
                for half in range(2):
                    by_core(z_forward)(k, half)
                for half in range(2):
                    by_core(z_last)(k, half)

        order = [name for name in ORDER if name in run]
        if len(order) < len(run):
            order = [f"{kind}{c}" for kind, count in (("i", 2), ("b", 1), ("g", in_parts), ("a", 1)) for c in range(count)]
            if group > 1:
                run["Z"] = z_all
                order.append("Z")
            for kinds in ("xy", "zo", "te", "f", "v", "wu", "h", "l", "n", "s", "m"):
                order += sorted((name for name in run if name[0] in kinds), key=lambda name: (name[1:], -ord(name[0])))
        for name in order:
            run[name]()

        if not streamed:
            k_step = 2 * LANES
            n_step = 4 * LANES

            def body(i, carry):
                ns = pl.ds(pl.multiple_of(i * n_step, n_step), n_step)
                acc[:, ns] = jnp.zeros((tok, n_step), F32)

                def inner(k, carry):
                    ks = pl.ds(pl.multiple_of(k * k_step, k_step), k_step)
                    acc[:, ns] += jnp.dot(act[:, ks], wall[ks, ns], preferred_element_type=F32)
                    return carry

                lax.fori_loop(0, width // k_step, inner, 0)
                out_v[0, :, ns] = acc[:, ns].astype(BF16)
                return carry

            lax.fori_loop(0, width // n_step, body, 0)

        ended = jnp.logical_or(s == 0, s == sp - 1)

        def finish(cc):
            left(sent[cc][0], send_sem.at[0])
            if sent[cc][1]:
                left(sent[cc][1], send_sem.at[2])
            for wanted, count in ((ended, 1), (jnp.logical_not(ended), sp + 1)):
                if sp > 1:
                    @pl.when(wanted)
                    def _():
                        left(count * (rows + (chips - 1) * late_rows[cc]) * cols, send_sem.at[1])

        by_core(finish)()

        @pl.when(s < sp - 1)
        def _():
            halo_copy.wait_send()

    scratch = [
        pltpu.VMEM((tok, width), BF16),
        pltpu.VMEM((tok, width), BF16),
        pltpu.VMEM((pad, width), BF16),
        pltpu.VMEM((pad, width), BF16),
        pltpu.VMEM((pad, width), BF16),
        pltpu.VMEM((pad, width), BF16),
        pltpu.VMEM((taps, width), BF16),
        pltpu.VMEM((taps, width), F32),
        pltpu.VMEM((1, width), F32),
        pltpu.VMEM((1, width), F32),
        pltpu.VMEM((pad + tok, width), F32),
        pltpu.VMEM((tok, width), F32),
        pltpu.VMEM((tok, width), BF16),
        pltpu.VMEM((tok, width), F32),
        pltpu.VMEM((dp * rows, sp * cols), BF16),
        pltpu.SemaphoreType.DMA((6 + 2 * in_parts,)),
        pltpu.SemaphoreType.DMA((2,)),
        pltpu.SemaphoreType.DMA((3,)),
        pltpu.SemaphoreType.DMA((2, sp)),
        pltpu.SemaphoreType.DMA((2, chips, parts)),
        pltpu.SemaphoreType.DMA((chips, sp) if group == 1 else (1, 1)),
        pltpu.SemaphoreType.DMA((chips, parts)),
    ]
    return kernel, scratch


def solution(mesh):
    sp, dp = mesh.shape["sp"], mesh.shape["dp"]
    chips = dp // 2
    xs = max(i for i in range(1, math.isqrt(chips) + 1) if chips % i == 0)
    ys = chips // xs
    parts = math.gcd(sp, max(1, 32 // dp))

    def per_device(value_half, gate_half, conv_taps, norm_gain, norm_shift, out_weight):
        _, tok, width = value_half.shape
        taps = conv_taps.shape[0]
        rows, cols = out_weight.shape
        pad = -(-(taps - 1) // 16) * 16
        kernel, scratch = make_kernel(sp, dp, xs, ys, parts, tok, width, taps, rows, cols, pad)
        return pl.pallas_call(
            kernel,
            out_shape=pltpu.VMEM(value_half.shape, BF16),
            in_specs=[pl.BlockSpec(memory_space=pltpu.HBM)] * 6,
            out_specs=pl.BlockSpec(memory_space=pltpu.VMEM),
            scratch_shapes=scratch,
            compiler_params=pltpu.CompilerParams(
                collective_id=0, has_side_effects=True, vmem_limit_bytes=VMEM_LIMIT),
        )(value_half, gate_half, conv_taps, norm_gain[None], norm_shift[None], out_weight)

    placed = (P("dp", "sp", None), P("dp", "sp", None), P(), P(), P(), P("dp", "sp"))
    return jax.shard_map(
        per_device, mesh=mesh, in_specs=placed, out_specs=P("dp", "sp", None), check_vma=False
    )
```

```python
import math
from functools import partial

import jax
import jax.numpy as jnp
from jax import lax
from jax.experimental import pallas as pl
from jax.experimental.pallas import tpu as pltpu
from jax.sharding import PartitionSpec as P

EPSILON = 1e-06
MESH = pl.DeviceIdType.MESH
F32 = jnp.float32
BF16 = jnp.bfloat16
LANES = 128
VMEM_LIMIT = 62 * 1024 * 1024
ORDER = (
    "i1", "x0", "o00", "b0", "t0", "o01", "y0", "g0", "i0", "g1", "a0", "e1", "e0", "z11", "z21", "o11",
    "z20", "z10", "g2", "v0", "o10", "f01", "y1", "z31", "h0", "o21", "s00", "o20", "l2", "s01", "v1", "g3",
    "l0", "f11", "w20", "z30", "w10", "u10", "v2", "f00", "e3", "o31", "l1", "v3", "e2", "w21", "l3", "w11",
    "u11", "w22", "f20", "o30", "n0", "w23", "w12", "n1", "s11", "s02", "f21", "s03", "m03", "f10", "s20", "s13",
    "w13", "m10", "u13", "m00", "w30", "u21", "u22", "f31", "s21", "w31", "w32", "u12", "f30", "w33", "m22", "u20",
    "s22", "s10", "s31", "m11", "u23", "m01", "m21", "m20", "u30", "s23", "s12", "m02", "m12", "u31", "m30", "m23",
    "u32", "s30", "s33", "m13", "s32", "u33", "m31", "m32", "m33",
)


def half_sigmoid(x):
    return 0.5 * jnp.tanh(0.5 * x) + 0.5


def nearest(me, count, k):
    place = jnp.int32(0)
    for here in range(count):
        there = sorted(range(count), key=lambda j: (abs(j - here), j))[k]
        place = place + jnp.where(me == here, there, 0).astype(jnp.int32)
    return place


def make_kernel(sp, dp, xs, ys, parts, tok, width, taps, rows, cols, pad):
    group = sp // parts
    part_cols = group * cols
    late_rows = [share // 8 * 8 if group == 1 else 0 for share in (rows * 7 // 32, rows * 6 // 32)]
    plane_start = (0, rows)
    half_rows, half_start = [], []
    for core_late, start, lean in zip(late_rows, plane_start, (4, 16)):
        one = (rows - core_late - (lean if core_late else 0)) // 2 // 8 * 8
        half_rows.append((one, rows - core_late - one))
        half_start.append((start + core_late, start + core_late + one))
    chips = xs * ys
    blocks = width // LANES
    row_chunk = 128 if tok % 128 == 0 else tok
    lead = pad - (taps - 1)
    in_parts = 4 if blocks % 4 == 0 else 1
    in_cols = width // in_parts
    streamed = rows % LANES == 0

    def kernel(v_hbm, g_hbm, taps_hbm, gain_hbm, shift_hbm, w_hbm, out_v,
               v_in, g_in, v_tail, g_tail, tail, halo, taps_in, taps_f, gain, shift, gated, conv, act, acc, wall,
               in_sem, halo_sem, send_sem, z_sem, recv_sem, late_sem, pair_sem):
        s = lax.axis_index("sp")
        d = lax.axis_index("dp")
        core = lax.rem(d, 2)
        x = lax.rem(d // 2, xs)
        y = d // (2 * xs)

        def index(yy, xx, cc):
            return (yy * xs + xx) * 2 + cc

        sibling = index(y, x, 1 - core)

        def along_x(step):
            return lax.rem(x + step, xs)

        def along_y(step):
            return lax.rem(y + step, ys)

        own = wall.at[pl.ds(pl.multiple_of(d * rows, rows), rows), pl.ds(pl.multiple_of(s * cols, cols), cols)]
        w_copy = pltpu.make_async_copy(w_hbm, own, in_sem.at[0])
        w_copy.start()
        tails = [
            pltpu.make_async_copy(src.at[0, pl.ds(tok - pad, pad), :], dst, in_sem.at[4])
            for src, dst in ((v_hbm, v_tail), (g_hbm, g_tail))
        ]
        for copy in tails:
            copy.start()
        loads = []
        for part in range(in_parts):
            sl = pl.ds(part * in_cols, in_cols)
            pair = (
                pltpu.make_async_copy(v_hbm.at[0, :, sl], v_in.at[:, sl], in_sem.at[5 + part]),
                pltpu.make_async_copy(g_hbm.at[0, :, sl], g_in.at[:, sl], in_sem.at[5 + part + in_parts % 4]),
            )
            loads.append(pair)
            for copy in pair:
                copy.start()
        small = [
            pltpu.make_async_copy(taps_hbm, taps_in, in_sem.at[1]),
            pltpu.make_async_copy(gain_hbm, gain, in_sem.at[2]),
            pltpu.make_async_copy(shift_hbm, shift, in_sem.at[3]),
        ]
        for copy in small:
            copy.start()

        barrier = pltpu.get_barrier_semaphore()
        friends = [(s, sibling)]
        friends += [(s, index(y, along_x(i), core)) for i in range(1, xs)]
        friends += [(s, index(along_y(i), x, core)) for i in range(1, ys)]
        for friend in friends:
            pl.semaphore_signal(barrier, inc=1, device_id=friend, device_id_type=MESH)
        above, below = s + 1 < sp, s > 0

        @pl.when(above)
        def _():
            pl.semaphore_signal(barrier, inc=1, device_id=(lax.rem(s + 1, sp), d), device_id_type=MESH)

        @pl.when(below)
        def _():
            pl.semaphore_signal(barrier, inc=1, device_id=(lax.rem(s + sp - 1, sp), d), device_id_type=MESH)

        pl.semaphore_wait(barrier, len(friends) + above.astype(jnp.int32) + below.astype(jnp.int32))
        w_copy.wait()

        me = d // 2
        sent = [[0, 0], [0, 0]]

        def by_core(act_on):
            def call(*where):
                for cc in range(2):
                    @pl.when(core == cc)
                    def _():
                        act_on(cc, *where)

            return call

        def send(cc, region, sem, target):
            copy = pltpu.make_async_remote_copy(
                src_ref=region, dst_ref=region, send_sem=send_sem.at[0], recv_sem=sem,
                device_id=(s, target), device_id_type=MESH)
            copy.start()
            sent[cc][0] += region.shape[0] * region.shape[1]

        def arrived(region, sem):
            pltpu.make_async_remote_copy(
                src_ref=region, dst_ref=region, send_sem=send_sem.at[0], recv_sem=sem,
                device_id=(s, sibling), device_id_type=MESH).wait_recv()

        def left(size, sem):
            units = size // LANES
            wide = max(j for j in range(1, blocks + 1) if units % (8 * j) == 0 and units // j <= dp * rows)
            region = wall.at[pl.ds(0, units // wide), pl.ds(0, wide * LANES)]
            pltpu.make_async_remote_copy(
                src_ref=region, dst_ref=region, send_sem=sem, recv_sem=pair_sem.at[0],
                device_id=(s, sibling), device_id_type=MESH).wait_send()

        def piece(chip, start, count, part):
            return wall.at[pl.ds(pl.multiple_of(chip * 2 * rows + start, 8), count),
                           pl.ds(pl.multiple_of(part * part_cols, part_cols), part_cols)]

        def block(cc, half, who):
            return wall.at[pl.ds(pl.multiple_of(me * 2 * rows + half_start[cc][half], 8), half_rows[cc][half]),
                           pl.ds(pl.multiple_of(who * cols, cols), cols)]

        def strip(cc, half, chip, part):
            return piece(chip, half_start[cc][half], half_rows[cc][half], part)

        def late_strip(cc, chip, who):
            return piece(chip, plane_start[cc], late_rows[cc], who)

        halo_copy = pltpu.make_async_remote_copy(
            src_ref=tail, dst_ref=halo, send_sem=halo_sem.at[0], recv_sem=halo_sem.at[1],
            device_id=(lax.rem(s + 1, sp), d), device_id_type=MESH)

        def send_halo():
            @pl.when(s < sp - 1)
            def _():
                halo_copy.start()

        def send_if(wanted, region, sem, target, column=None):
            copy = pltpu.make_async_remote_copy(
                src_ref=region, dst_ref=region, send_sem=send_sem.at[1 if column is None else 2], recv_sem=sem,
                device_id=(target, d if column is None else column), device_id_type=MESH)

            @pl.when(wanted)
            def _():
                copy.start()

        def z_sends(cc, half):
            send_if(s + 1 < sp, block(cc, half, s), z_sem.at[half, s], lax.rem(s + 1, sp))
            send_if(s > 0, block(cc, half, s), z_sem.at[half, s], lax.rem(s + sp - 1, sp))

        def z_link(k):
            source = nearest(s, sp, k)
            target = jnp.where(source < s, s + 1, s - 1)
            onward = jnp.logical_and(target >= 0, target < sp)
            return source, lax.rem(target + sp, sp), onward

        def z_forward(cc, k, half):
            source, target, onward = z_link(k)

            @pl.when(onward)
            def _():
                arrived(block(cc, half, source), z_sem.at[half, source])

            send_if(onward, block(cc, half, source), z_sem.at[half, source], target)

        def z_last(cc, k, half):
            source, _, onward = z_link(k)

            @pl.when(jnp.logical_not(onward))
            def _():
                arrived(block(cc, half, source), z_sem.at[half, source])

        my_part = s // group
        part_of = [nearest(my_part, parts, k) for k in range(parts)]

        def chip_at(fx, fy):
            return along_y(fy) * xs + along_x(fx)

        def firsts(half):
            if half == 0:
                return list(range(1, xs))
            return [xs * i for i in range(1, ys)]

        def slot(c, i, half):
            return recv_sem.at[(c * (chips - 1) + i - 1) * 2 + half]

        def pair(c, i):
            return pair_sem.at[(c - 1) * chips + i + 1 if c else 0]

        def hand_over(cc, c, i, half, j, region):
            fx, fy, tx, ty = i % xs, i // xs, j % xs, j // xs
            seen = (fy - ty) % ys * xs + (fx - tx) % xs
            send(cc, region, slot(c, seen, half), 2 * mine(j) + cc)

        def event_own(cc, c, half):
            part = part_of[c]
            if group == 1 and c > 0:
                z_last(cc, c, half)
            region = strip(cc, half, me, part)
            for j in firsts(half) + firsts(1 - half):
                hand_over(cc, c, 0, half, j, region)
            send(cc, region, pair(c, 0), sibling)

        def event_first(cc, c, half):
            for i in firsts(half):
                region = strip(cc, half, mine(i), part_of[c])
                arrived(region, slot(c, i, half))
                for j in firsts(1 - half):
                    hand_over(cc, c, i, half, j, region)
                send(cc, region, pair(c, i), sibling)

        seconds = []
        for one in range(max(xs, ys)):
            for two in range(1, max(xs, ys)):
                for half in range(2):
                    fx, fy = (one, two) if half == 0 else (two, one)
                    if fx < xs and fy < ys:
                        seconds.append((half, fx, fy))

        def event_second(cc, c, q):
            half, fx, fy = seconds[q]
            i = fy * xs + fx
            region = strip(cc, half, mine(i), part_of[c])
            arrived(region, slot(c, i, half))
            send(cc, region, pair(c, i), sibling)

        def mine(i):
            return chip_at(i % xs, i // xs)

        def late_x(cc):
            for i in range(1, xs):
                send(cc, late_strip(cc, me, s), late_sem.at[me, s], 2 * mine(i) + cc)

        def late_y(cc, c):
            for i in range(1, xs) if c else (0,):
                region, sem = late_strip(cc, mine(i), s), late_sem.at[mine(i), s]
                if i:
                    arrived(region, sem)
                for j in range(1, ys):
                    send(cc, region, sem, 2 * chip_at(0, j) + cc)

        def late_z(cc, i):
            region, sem = late_strip(cc, mine(i), s), late_sem.at[mine(i), s]
            if i >= xs:
                arrived(region, sem)
            send_if(s + 1 < sp, region, sem, lax.rem(s + 1, sp))
            send_if(s > 0, region, sem, lax.rem(s + sp - 1, sp))
            send(cc, region, pair(0, i), sibling)

        def late_forward(cc, k, i):
            source, target, onward = z_link(k)
            region, sem = late_strip(cc, mine(i), source), late_sem.at[mine(i), source]

            @pl.when(onward)
            def _():
                arrived(region, sem)

            send_if(onward, region, sem, target)
            send_if(onward, region, pair(k, i), s, sibling)

        def late_last(cc, k, i):
            source, _, onward = z_link(k)
            ended = jnp.logical_not(onward)
            region, sem = late_strip(cc, mine(i), source), late_sem.at[mine(i), source]

            @pl.when(ended)
            def _():
                arrived(region, sem)

            send_if(ended, region, pair(k, i), s, sibling)
            sent[cc][1] += region.shape[0] * region.shape[1]

        def gate_tail():
            two = pl.ds(0, 2 * pad)
            pltpu.make_async_copy(v_hbm.at[0, two, :], v_in.at[two, :], in_sem.at[4]).wait()

            def body(j, carry):
                cs = pl.ds(pl.multiple_of(j * LANES, LANES), LANES)
                tail[:, cs] = (v_tail[:, cs].astype(F32) * half_sigmoid(g_tail[:, cs].astype(F32))).astype(BF16)
                return carry

            lax.fori_loop(0, blocks, body, 0)

        def gated_rows(part):
            if in_parts == 1:
                for copy in loads[part]:
                    copy.wait()
            else:
                two = pl.ds(0, 2 * in_cols)
                pltpu.make_async_copy(v_hbm.at[0, :, two], v_in.at[:, two], in_sem.at[5 + part]).wait()

            def body(j, carry):
                cs = pl.ds(pl.multiple_of(part * in_cols + j * LANES, LANES), LANES)
                value = v_in[:, cs].astype(F32)
                gate = g_in[:, cs].astype(F32)
                gated[pl.ds(pad, tok), cs] = (value * half_sigmoid(gate)).astype(BF16).astype(F32)
                return carry

            lax.fori_loop(0, in_cols // LANES, body, 0)

        def taps_up():
            for copy in small:
                copy.wait()
            taps_f[...] = taps_in[...].astype(F32)

        def halo_rows():
            @pl.when(s == 0)
            def _():
                gated[pl.ds(0, pad), :] = jnp.zeros((pad, width), F32)

            @pl.when(s > 0)
            def _():
                halo_copy.wait_recv()

                def body(j, carry):
                    cs = pl.ds(pl.multiple_of(j * LANES, LANES), LANES)
                    gated[pl.ds(0, pad), cs] = halo[:, cs].astype(F32)
                    return carry

                lax.fori_loop(0, blocks, body, 0)

        def mix(row_starts, lo, hi):
            def body(j, carry):
                cs = pl.ds(pl.multiple_of(j * LANES, LANES), LANES)
                for start in row_starts:
                    seen = gated[pl.ds(start, row_chunk + pad), cs]
                    total = None
                    for r in range(8):
                        inner = None
                        length = row_chunk + (8 if r else 0)
                        for q in range(0, pad // 8 + 1):
                            tap = 8 * q + r - lead
                            if 0 <= tap < taps:
                                term = seen[8 * q:8 * q + length] * taps_f[pl.ds(tap, 1), cs]
                                inner = term if inner is None else inner + term
                        if inner is None:
                            continue
                        if r:
                            inner = pltpu.roll(inner, length - r, 0)[:row_chunk]
                        total = inner if total is None else total + inner
                    conv[pl.ds(start, row_chunk), cs] = total.astype(BF16).astype(F32)
                return carry

            lax.fori_loop(lo, hi, body, 0)

        def normalise(low, high):
            step = math.gcd(64, row_chunk)

            def body(i, carry):
                rs = pl.ds(pl.multiple_of(i * step, step), step)
                columns = [slice(j * LANES, (j + 1) * LANES) for j in range(blocks)]
                total = conv[rs, columns[0]]
                for cs in columns[1:]:
                    total = total + conv[rs, cs]
                mean = jnp.sum(total, axis=1, keepdims=True) * (1.0 / width)
                mean = jnp.broadcast_to(mean, (step, LANES))
                total = jnp.zeros((step, LANES), F32)
                for cs in columns:
                    centered = conv[rs, cs] - mean
                    total = total + centered * centered
                variance = jnp.sum(total, axis=1, keepdims=True) * (1.0 / width)
                scale = jnp.broadcast_to(lax.rsqrt(variance + EPSILON), (step, LANES))
                for cs in columns:
                    half = (conv[rs, cs] - mean) * scale * (0.5 * gain[:, cs]) + 0.5 * shift[:, cs]
                    act[rs, cs] = (half * jnp.tanh(half) + half).astype(BF16)
                return carry

            lax.fori_loop(low // step, high // step, body, 0)

        multiplied = [0] * parts

        def sibling_strip(cc, c, i):
            if c:
                arrived(piece(mine(i), plane_start[1 - cc], rows, part_of[c]), pair(c, i))
            elif multiplied[0] == 0:
                arrived(piece(0, 0, chips * rows, part_of[c]), pair(c, i))

        def multiply(c, i):
            part = part_of[c]
            by_core(sibling_strip)(c, i)
            multiplied[c] += 1
            if not streamed:
                return
            ks = pl.ds(pl.multiple_of(mine(i) * 2 * rows, 2 * rows), 2 * rows)
            ns = pl.ds(pl.multiple_of(part * part_cols, part_cols), part_cols)
            term = jnp.dot(act[:, ks], wall[ks, ns], preferred_element_type=F32)
            if multiplied[c] == 1:
                acc[:, ns] = term
            elif multiplied[c] < chips:
                acc[:, ns] += term
            else:
                out_v[0, :, ns] = (acc[:, ns] + term).astype(BF16)

        early = [start for start in range(0, tok, row_chunk) if start >= pad]
        late = [start for start in range(0, tok, row_chunk) if start < pad]

        edges = [blocks * i // 4 for i in range(5)]
        small_step = {
            "g": (gated_rows, in_parts),
            "e": (lambda c: mix(early, edges[c], edges[c + 1]), 4),
            "l": (lambda c: mix(late, edges[c], edges[c + 1]), 4),
            "n": (lambda c: normalise(*((late[-1] + row_chunk, tok), (0, late[-1] + row_chunk))[c]), 2),
        }
        run = {
            "t0": taps_up,
            "b0": gate_tail,
            "a0": send_halo,
            "h0": halo_rows,
        }
        for kind, (act_on, count) in small_step.items():
            for c in range(count):
                run[f"{kind}{c}"] = partial(act_on, c)
        for half in range(2):
            run[f"i{half}"] = partial(by_core(z_sends), half)
            if group == 1:
                for k in range(1, sp):
                    run[f"z{k}{half}"] = partial(by_core(z_forward), k, half)
        for c in range(parts):
            for half in range(2):
                run[f"o{c}{half}"] = partial(by_core(event_own), c, half)
                run[f"f{c}{half}"] = partial(by_core(event_first), c, half)
            for q in range(len(seconds)):
                run[f"s{c}{q}"] = partial(by_core(event_second), c, q)
            for i in range(chips):
                run[f"m{c}{i}"] = partial(multiply, c, i)
        if group == 1:
            run["x0"] = by_core(late_x)
            run["y0"] = partial(by_core(late_y), 0)
            run["y1"] = partial(by_core(late_y), 1)
            for i in range(chips):
                run[f"v{i}"] = partial(by_core(late_z), i)
                for k in range(1, sp):
                    run[f"w{k}{i}"] = partial(by_core(late_forward), k, i)
                    run[f"u{k}{i}"] = partial(by_core(late_last), k, i)

        def z_all():
            for k in range(1, sp):
                for half in range(2):
                    by_core(z_forward)(k, half)
                for half in range(2):
                    by_core(z_last)(k, half)

        order = [name for name in ORDER if name in run]
        if len(order) < len(run):
            order = [f"{kind}{c}" for kind, count in (("i", 2), ("b", 1), ("g", in_parts), ("a", 1)) for c in range(count)]
            if group > 1:
                run["Z"] = z_all
                order.append("Z")
            for kinds in ("xy", "zo", "te", "f", "v", "wu", "h", "l", "n", "s", "m"):
                order += sorted((name for name in run if name[0] in kinds), key=lambda name: (name[1:], -ord(name[0])))
        for name in order:
            run[name]()

        if not streamed:
            k_step = 2 * LANES
            n_step = 4 * LANES

            def body(i, carry):
                ns = pl.ds(pl.multiple_of(i * n_step, n_step), n_step)
                acc[:, ns] = jnp.zeros((tok, n_step), F32)

                def inner(k, carry):
                    ks = pl.ds(pl.multiple_of(k * k_step, k_step), k_step)
                    acc[:, ns] += jnp.dot(act[:, ks], wall[ks, ns], preferred_element_type=F32)
                    return carry

                lax.fori_loop(0, width // k_step, inner, 0)
                out_v[0, :, ns] = acc[:, ns].astype(BF16)
                return carry

            lax.fori_loop(0, width // n_step, body, 0)

        ended = jnp.logical_or(s == 0, s == sp - 1)

        def finish(cc):
            left(sent[cc][0], send_sem.at[0])
            if sent[cc][1]:
                left(sent[cc][1], send_sem.at[2])
            for wanted, count in ((ended, 1), (jnp.logical_not(ended), sp + 1)):
                if sp > 1:
                    @pl.when(wanted)
                    def _():
                        left(count * (rows + (chips - 1) * late_rows[cc]) * cols, send_sem.at[1])

        by_core(finish)()

        @pl.when(s < sp - 1)
        def _():
            halo_copy.wait_send()

    scratch = [
        pltpu.VMEM((tok, width), BF16),
        pltpu.VMEM((tok, width), BF16),
        pltpu.VMEM((pad, width), BF16),
        pltpu.VMEM((pad, width), BF16),
        pltpu.VMEM((pad, width), BF16),
        pltpu.VMEM((pad, width), BF16),
        pltpu.VMEM((taps, width), BF16),
        pltpu.VMEM((taps, width), F32),
        pltpu.VMEM((1, width), F32),
        pltpu.VMEM((1, width), F32),
        pltpu.VMEM((pad + tok, width), F32),
        pltpu.VMEM((tok, width), F32),
        pltpu.VMEM((tok, width), BF16),
        pltpu.VMEM((tok, width), F32),
        pltpu.VMEM((dp * rows, sp * cols), BF16),
        pltpu.SemaphoreType.DMA((5 + max(in_parts, 2),)),
        pltpu.SemaphoreType.DMA((2,)),
        pltpu.SemaphoreType.DMA((3,)),
        pltpu.SemaphoreType.DMA((2, sp)),
        pltpu.SemaphoreType.DMA((parts * (chips - 1) * 2,)),
        pltpu.SemaphoreType.DMA((chips, sp) if group == 1 else (1, 1)),
        pltpu.SemaphoreType.DMA(((parts - 1) * chips + 1,)),
    ]
    return kernel, scratch


def solution(mesh):
    sp, dp = mesh.shape["sp"], mesh.shape["dp"]
    chips = dp // 2
    xs = max(i for i in range(1, math.isqrt(chips) + 1) if chips % i == 0)
    ys = chips // xs
    parts = math.gcd(sp, max(1, 32 // dp))

    def per_device(value_half, gate_half, conv_taps, norm_gain, norm_shift, out_weight):
        _, tok, width = value_half.shape
        taps = conv_taps.shape[0]
        rows, cols = out_weight.shape
        pad = -(-(taps - 1) // 16) * 16
        kernel, scratch = make_kernel(sp, dp, xs, ys, parts, tok, width, taps, rows, cols, pad)
        return pl.pallas_call(
            kernel,
            out_shape=pltpu.VMEM(value_half.shape, BF16),
            in_specs=[pl.BlockSpec(memory_space=pltpu.HBM)] * 6,
            out_specs=pl.BlockSpec(memory_space=pltpu.VMEM),
            scratch_shapes=scratch,
            compiler_params=pltpu.CompilerParams(
                collective_id=0, has_side_effects=True, vmem_limit_bytes=VMEM_LIMIT),
        )(value_half, gate_half, conv_taps, norm_gain[None], norm_shift[None], out_weight)

    placed = (P("dp", "sp", None), P("dp", "sp", None), P(), P(), P(), P("dp", "sp"))
    return jax.shard_map(
        per_device, mesh=mesh, in_specs=placed, out_specs=P("dp", "sp", None), check_vma=False
    )
```

```python
import math
from functools import partial

import jax
import jax.numpy as jnp
from jax import lax
from jax.experimental import pallas as pl
from jax.experimental.pallas import tpu as pltpu
from jax.sharding import PartitionSpec as P

EPSILON = 1e-06
MESH = pl.DeviceIdType.MESH
F32 = jnp.float32
BF16 = jnp.bfloat16
LANES = 128
VMEM_LIMIT = 62 * 1024 * 1024
ORDER = (
    "i1", "x0", "o01", "t0", "o00", "g3", "y0", "i0", "y1", "v0", "z11", "o11", "z21", "b0", "e3", "g1",
    "g0", "z10", "g2", "a0", "z20", "f01", "e0", "o10", "f00", "v1", "s11", "z31", "w20", "v2", "f11", "e1",
    "s00", "o21", "e2", "z30", "v3", "o20", "h0", "w10", "f10", "u11", "w21", "s03", "l2", "w12", "w22", "s01",
    "u10", "w11", "l1", "l0", "l3", "o31", "n1", "n0", "m10", "w23", "o30", "s02", "m03", "s20", "m01", "f20",
    "f21", "w32", "s10", "w31", "u20", "w13", "s31", "u13", "m00", "w30", "u21", "s12", "s13", "f31", "m20", "u22",
    "f30", "w33", "s21", "u12", "m11", "m22", "s30", "m21", "u32", "s23", "u31", "m12", "m02", "u23", "s22", "m31",
    "m13", "u30", "m32", "s33", "s32", "u33", "m23", "m30", "m33",
)


def half_sigmoid(x):
    return 0.5 * jnp.tanh(0.5 * x) + 0.5


def nearest(me, count, k):
    place = jnp.int32(0)
    for here in range(count):
        there = sorted(range(count), key=lambda j: (abs(j - here), j))[k]
        place = place + jnp.where(me == here, there, 0).astype(jnp.int32)
    return place


def make_kernel(sp, dp, xs, ys, parts, tok, width, taps, rows, cols, pad):
    group = sp // parts
    part_cols = group * cols
    late_rows = [share // 8 * 8 if group == 1 else 0 for share in (rows * 7 // 32, rows * 6 // 32)]
    plane_start = (0, rows)
    half_rows, half_start = [], []
    for core_late, start, lean in zip(late_rows, plane_start, (4, 16)):
        one = (rows - core_late - (lean if core_late else 0)) // 2 // 8 * 8
        half_rows.append((one, rows - core_late - one))
        half_start.append((start + core_late, start + core_late + one))
    chips = xs * ys
    blocks = width // LANES
    row_chunk = 128 if tok % 128 == 0 else tok
    lead = pad - (taps - 1)
    in_parts = 4 if blocks % 4 == 0 else 1
    in_cols = width // in_parts
    streamed = rows % LANES == 0

    def kernel(v_hbm, g_hbm, taps_hbm, gain_hbm, shift_hbm, w_hbm, out_v,
               v_in, g_in, v_tail, g_tail, tail, halo, taps_in, taps_f, gain, shift, gated, conv, act, acc, wall,
               in_sem, halo_sem, send_sem, z_sem, recv_sem, late_sem, pair_sem):
        s = lax.axis_index("sp")
        d = lax.axis_index("dp")
        core = lax.rem(d, 2)
        x = lax.rem(d // 2, xs)
        y = d // (2 * xs)

        def index(yy, xx, cc):
            return (yy * xs + xx) * 2 + cc

        sibling = index(y, x, 1 - core)

        def along_x(step):
            return lax.rem(x + step, xs)

        def along_y(step):
            return lax.rem(y + step, ys)

        own = wall.at[pl.ds(pl.multiple_of(d * rows, rows), rows), pl.ds(pl.multiple_of(s * cols, cols), cols)]
        w_copy = pltpu.make_async_copy(w_hbm, own, in_sem.at[0])
        w_copy.start()
        tails = [
            pltpu.make_async_copy(src.at[0, pl.ds(tok - pad, pad), :], dst, in_sem.at[4])
            for src, dst in ((v_hbm, v_tail), (g_hbm, g_tail))
        ]
        for copy in tails:
            copy.start()
        loads = []
        for part in range(in_parts):
            sl = pl.ds(part * in_cols, in_cols)
            pair = (
                pltpu.make_async_copy(v_hbm.at[0, :, sl], v_in.at[:, sl], in_sem.at[5 + part]),
                pltpu.make_async_copy(g_hbm.at[0, :, sl], g_in.at[:, sl], in_sem.at[5 + part + in_parts % 4]),
            )
            loads.append(pair)
            for copy in pair:
                copy.start()
        small = [
            pltpu.make_async_copy(taps_hbm, taps_in, in_sem.at[1]),
            pltpu.make_async_copy(gain_hbm, gain, in_sem.at[2]),
            pltpu.make_async_copy(shift_hbm, shift, in_sem.at[3]),
        ]
        for copy in small:
            copy.start()

        barrier = pltpu.get_barrier_semaphore()
        friends = [(s, sibling)]
        friends += [(s, index(y, along_x(i), core)) for i in range(1, xs)]
        friends += [(s, index(along_y(i), x, core)) for i in range(1, ys)]
        for friend in friends:
            pl.semaphore_signal(barrier, inc=1, device_id=friend, device_id_type=MESH)
        above, below = s + 1 < sp, s > 0

        @pl.when(above)
        def _():
            pl.semaphore_signal(barrier, inc=1, device_id=(lax.rem(s + 1, sp), d), device_id_type=MESH)

        @pl.when(below)
        def _():
            pl.semaphore_signal(barrier, inc=1, device_id=(lax.rem(s + sp - 1, sp), d), device_id_type=MESH)

        pl.semaphore_wait(barrier, len(friends) + above.astype(jnp.int32) + below.astype(jnp.int32))
        w_copy.wait()

        me = d // 2
        sent = [[0, 0], [0, 0]]

        def by_core(act_on):
            def call(*where):
                for cc in range(2):
                    @pl.when(core == cc)
                    def _():
                        act_on(cc, *where)

            return call

        def send(cc, region, sem, target):
            copy = pltpu.make_async_remote_copy(
                src_ref=region, dst_ref=region, send_sem=send_sem.at[0], recv_sem=sem,
                device_id=(s, target), device_id_type=MESH)
            copy.start()
            sent[cc][0] += region.shape[0] * region.shape[1]

        def arrived(region, sem):
            pltpu.make_async_remote_copy(
                src_ref=region, dst_ref=region, send_sem=send_sem.at[0], recv_sem=sem,
                device_id=(s, sibling), device_id_type=MESH).wait_recv()

        def left(size, sem):
            units = size // LANES
            wide = max(j for j in range(1, blocks + 1) if units % (8 * j) == 0 and units // j <= dp * rows)
            region = wall.at[pl.ds(0, units // wide), pl.ds(0, wide * LANES)]
            pltpu.make_async_remote_copy(
                src_ref=region, dst_ref=region, send_sem=sem, recv_sem=pair_sem.at[0],
                device_id=(s, sibling), device_id_type=MESH).wait_send()

        def piece(chip, start, count, part):
            return wall.at[pl.ds(pl.multiple_of(chip * 2 * rows + start, 8), count),
                           pl.ds(pl.multiple_of(part * part_cols, part_cols), part_cols)]

        def block(cc, half, who):
            return wall.at[pl.ds(pl.multiple_of(me * 2 * rows + half_start[cc][half], 8), half_rows[cc][half]),
                           pl.ds(pl.multiple_of(who * cols, cols), cols)]

        def strip(cc, half, chip, part):
            return piece(chip, half_start[cc][half], half_rows[cc][half], part)

        def late_strip(cc, chip, who):
            return piece(chip, plane_start[cc], late_rows[cc], who)

        halo_copy = pltpu.make_async_remote_copy(
            src_ref=tail, dst_ref=halo, send_sem=halo_sem.at[0], recv_sem=halo_sem.at[1],
            device_id=(lax.rem(s + 1, sp), d), device_id_type=MESH)

        def send_halo():
            @pl.when(s < sp - 1)
            def _():
                halo_copy.start()

        def send_if(wanted, region, sem, target, column=None):
            copy = pltpu.make_async_remote_copy(
                src_ref=region, dst_ref=region, send_sem=send_sem.at[1 if column is None else 2], recv_sem=sem,
                device_id=(target, d if column is None else column), device_id_type=MESH)

            @pl.when(wanted)
            def _():
                copy.start()

        def z_sends(cc, half):
            send_if(s + 1 < sp, block(cc, half, s), z_sem.at[half, s], lax.rem(s + 1, sp))
            send_if(s > 0, block(cc, half, s), z_sem.at[half, s], lax.rem(s + sp - 1, sp))

        def z_link(k):
            source = nearest(s, sp, k)
            target = jnp.where(source < s, s + 1, s - 1)
            onward = jnp.logical_and(target >= 0, target < sp)
            return source, lax.rem(target + sp, sp), onward

        def z_forward(cc, k, half):
            source, target, onward = z_link(k)

            @pl.when(onward)
            def _():
                arrived(block(cc, half, source), z_sem.at[half, source])

            send_if(onward, block(cc, half, source), z_sem.at[half, source], target)

        def z_last(cc, k, half):
            source, _, onward = z_link(k)

            @pl.when(jnp.logical_not(onward))
            def _():
                arrived(block(cc, half, source), z_sem.at[half, source])

        my_part = s // group
        part_of = [nearest(my_part, parts, k) for k in range(parts)]

        def chip_at(fx, fy):
            return along_y(fy) * xs + along_x(fx)

        def firsts(half):
            if half == 0:
                return list(range(1, xs))
            return [xs * i for i in range(1, ys)]

        def slot(c, i, half):
            return recv_sem.at[(c * (chips - 1) + i - 1) * 2 + half]

        def pair(c, i):
            return pair_sem.at[(c - 1) * chips + i + 1 if c else 0]

        def hand_over(cc, c, i, half, j, region):
            fx, fy, tx, ty = i % xs, i // xs, j % xs, j // xs
            seen = (fy - ty) % ys * xs + (fx - tx) % xs
            send(cc, region, slot(c, seen, half), 2 * mine(j) + cc)

        def event_own(cc, c, half):
            part = part_of[c]
            if group == 1 and c > 0:
                z_last(cc, c, half)
            region = strip(cc, half, me, part)
            for j in firsts(half) + firsts(1 - half):
                hand_over(cc, c, 0, half, j, region)
            send(cc, region, pair(c, 0), sibling)

        def event_first(cc, c, half):
            for i in firsts(half):
                region = strip(cc, half, mine(i), part_of[c])
                arrived(region, slot(c, i, half))
                for j in firsts(1 - half):
                    hand_over(cc, c, i, half, j, region)
                send(cc, region, pair(c, i), sibling)

        seconds = []
        for one in range(max(xs, ys)):
            for two in range(1, max(xs, ys)):
                for half in range(2):
                    fx, fy = (one, two) if half == 0 else (two, one)
                    if fx < xs and fy < ys:
                        seconds.append((half, fx, fy))

        def event_second(cc, c, q):
            half, fx, fy = seconds[q]
            i = fy * xs + fx
            region = strip(cc, half, mine(i), part_of[c])
            arrived(region, slot(c, i, half))
            send(cc, region, pair(c, i), sibling)

        def mine(i):
            return chip_at(i % xs, i // xs)

        def late_x(cc):
            for i in range(1, xs):
                send(cc, late_strip(cc, me, s), late_sem.at[me, s], 2 * mine(i) + cc)

        def late_y(cc, c):
            for i in range(1, xs) if c else (0,):
                region, sem = late_strip(cc, mine(i), s), late_sem.at[mine(i), s]
                if i:
                    arrived(region, sem)
                for j in range(1, ys):
                    send(cc, region, sem, 2 * chip_at(0, j) + cc)

        def late_z(cc, i):
            region, sem = late_strip(cc, mine(i), s), late_sem.at[mine(i), s]
            if i >= xs:
                arrived(region, sem)
            send_if(s + 1 < sp, region, sem, lax.rem(s + 1, sp))
            send_if(s > 0, region, sem, lax.rem(s + sp - 1, sp))
            send(cc, region, pair(0, i), sibling)

        def late_forward(cc, k, i):
            source, target, onward = z_link(k)
            region, sem = late_strip(cc, mine(i), source), late_sem.at[mine(i), source]

            @pl.when(onward)
            def _():
                arrived(region, sem)

            send_if(onward, region, sem, target)
            send_if(onward, region, pair(k, i), s, sibling)

        def late_last(cc, k, i):
            source, _, onward = z_link(k)
            ended = jnp.logical_not(onward)
            region, sem = late_strip(cc, mine(i), source), late_sem.at[mine(i), source]

            @pl.when(ended)
            def _():
                arrived(region, sem)

            send_if(ended, region, pair(k, i), s, sibling)
            sent[cc][1] += region.shape[0] * region.shape[1]

        def gate_tail():
            two = pl.ds(0, 2 * pad)
            pltpu.make_async_copy(v_hbm.at[0, two, :], v_in.at[two, :], in_sem.at[4]).wait()

            def body(j, carry):
                cs = pl.ds(pl.multiple_of(j * LANES, LANES), LANES)
                tail[:, cs] = (v_tail[:, cs].astype(F32) * half_sigmoid(g_tail[:, cs].astype(F32))).astype(BF16)
                return carry

            lax.fori_loop(0, blocks, body, 0)

        def gated_rows(part):
            if in_parts == 1:
                for copy in loads[part]:
                    copy.wait()
            else:
                two = pl.ds(0, 2 * in_cols)
                pltpu.make_async_copy(v_hbm.at[0, :, two], v_in.at[:, two], in_sem.at[5 + part]).wait()

            def body(j, carry):
                cs = pl.ds(pl.multiple_of(part * in_cols + j * LANES, LANES), LANES)
                value = v_in[:, cs].astype(F32)
                gate = g_in[:, cs].astype(F32)
                gated[pl.ds(pad, tok), cs] = (value * half_sigmoid(gate)).astype(BF16).astype(F32)
                return carry

            lax.fori_loop(0, in_cols // LANES, body, 0)

        def taps_up():
            for copy in small:
                copy.wait()
            taps_f[...] = taps_in[...].astype(F32)

        def halo_rows():
            @pl.when(s == 0)
            def _():
                gated[pl.ds(0, pad), :] = jnp.zeros((pad, width), F32)

            @pl.when(s > 0)
            def _():
                halo_copy.wait_recv()

                def body(j, carry):
                    cs = pl.ds(pl.multiple_of(j * LANES, LANES), LANES)
                    gated[pl.ds(0, pad), cs] = halo[:, cs].astype(F32)
                    return carry

                lax.fori_loop(0, blocks, body, 0)

        def mix(row_starts, lo, hi):
            def body(j, carry):
                cs = pl.ds(pl.multiple_of(j * LANES, LANES), LANES)
                for start in row_starts:
                    seen = gated[pl.ds(start, row_chunk + pad), cs]
                    total = None
                    for r in range(8):
                        inner = None
                        length = row_chunk + (8 if r else 0)
                        for q in range(0, pad // 8 + 1):
                            tap = 8 * q + r - lead
                            if 0 <= tap < taps:
                                term = seen[8 * q:8 * q + length] * taps_f[pl.ds(tap, 1), cs]
                                inner = term if inner is None else inner + term
                        if inner is None:
                            continue
                        if r:
                            inner = pltpu.roll(inner, length - r, 0)[:row_chunk]
                        total = inner if total is None else total + inner
                    conv[pl.ds(start, row_chunk), cs] = total.astype(BF16).astype(F32)
                return carry

            lax.fori_loop(lo, hi, body, 0)

        def normalise(low, high):
            step = math.gcd(64, row_chunk)

            def body(i, carry):
                rs = pl.ds(pl.multiple_of(i * step, step), step)
                columns = [slice(j * LANES, (j + 1) * LANES) for j in range(blocks)]
                total = conv[rs, columns[0]]
                for cs in columns[1:]:
                    total = total + conv[rs, cs]
                mean = jnp.sum(total, axis=1, keepdims=True) * (1.0 / width)
                mean = jnp.broadcast_to(mean, (step, LANES))
                total = jnp.zeros((step, LANES), F32)
                for cs in columns:
                    centered = conv[rs, cs] - mean
                    total = total + centered * centered
                variance = jnp.sum(total, axis=1, keepdims=True) * (1.0 / width)
                scale = jnp.broadcast_to(lax.rsqrt(variance + EPSILON), (step, LANES))
                for cs in columns:
                    half = (conv[rs, cs] - mean) * scale * (0.5 * gain[:, cs]) + 0.5 * shift[:, cs]
                    act[rs, cs] = (half * jnp.tanh(half) + half).astype(BF16)
                return carry

            lax.fori_loop(low // step, high // step, body, 0)

        multiplied = [0] * parts

        def sibling_strip(cc, c, i):
            if c:
                arrived(piece(mine(i), plane_start[1 - cc], rows, part_of[c]), pair(c, i))
            elif multiplied[0] == 0:
                arrived(piece(0, 0, chips * rows, part_of[c]), pair(c, i))

        def product(c, i, start, count):
            part = part_of[c]
            ks = pl.ds(pl.multiple_of(mine(i) * 2 * rows + start, count), count)
            ns = pl.ds(pl.multiple_of(part * part_cols, part_cols), part_cols)
            return ns, jnp.dot(act[:, ks], wall[ks, ns], preferred_element_type=F32)

        def multiply(c, i, last):
            if last:
                ns, term = product(c, i, core * rows, rows)
                acc[:, ns] += term
            by_core(sibling_strip)(c, i)
            multiplied[c] += 1
            if not streamed:
                return
            ns, term = product(c, i, (1 - core) * rows, rows) if last else product(c, i, 0, 2 * rows)
            if multiplied[c] == 1:
                acc[:, ns] = term
            elif multiplied[c] < chips:
                acc[:, ns] += term
            else:
                out_v[0, :, ns] = (acc[:, ns] + term).astype(BF16)

        early = [start for start in range(0, tok, row_chunk) if start >= pad]
        late = [start for start in range(0, tok, row_chunk) if start < pad]

        edges = [blocks * i // 4 for i in range(5)]
        small_step = {
            "g": (gated_rows, in_parts),
            "e": (lambda c: mix(early, edges[c], edges[c + 1]), 4),
            "l": (lambda c: mix(late, edges[c], edges[c + 1]), 4),
            "n": (lambda c: normalise(*((late[-1] + row_chunk, tok), (0, late[-1] + row_chunk))[c]), 2),
        }
        ending = [name for name in ORDER if name[0] == "m"][-2:] if streamed and group == 1 and chips > 2 else []
        run = {
            "t0": taps_up,
            "b0": gate_tail,
            "a0": send_halo,
            "h0": halo_rows,
        }
        for kind, (act_on, count) in small_step.items():
            for c in range(count):
                run[f"{kind}{c}"] = partial(act_on, c)
        for half in range(2):
            run[f"i{half}"] = partial(by_core(z_sends), half)
            if group == 1:
                for k in range(1, sp):
                    run[f"z{k}{half}"] = partial(by_core(z_forward), k, half)
        for c in range(parts):
            for half in range(2):
                run[f"o{c}{half}"] = partial(by_core(event_own), c, half)
                run[f"f{c}{half}"] = partial(by_core(event_first), c, half)
            for q in range(len(seconds)):
                run[f"s{c}{q}"] = partial(by_core(event_second), c, q)
            for i in range(chips):
                run[f"m{c}{i}"] = partial(multiply, c, i, f"m{c}{i}" in ending)
        if group == 1:
            run["x0"] = by_core(late_x)
            run["y0"] = partial(by_core(late_y), 0)
            run["y1"] = partial(by_core(late_y), 1)
            for i in range(chips):
                run[f"v{i}"] = partial(by_core(late_z), i)
                for k in range(1, sp):
                    run[f"w{k}{i}"] = partial(by_core(late_forward), k, i)
                    run[f"u{k}{i}"] = partial(by_core(late_last), k, i)

        def z_all():
            for k in range(1, sp):
                for half in range(2):
                    by_core(z_forward)(k, half)
                for half in range(2):
                    by_core(z_last)(k, half)

        order = [name for name in ORDER if name in run]
        if len(order) < len(run):
            order = [f"{kind}{c}" for kind, count in (("i", 2), ("b", 1), ("g", in_parts), ("a", 1)) for c in range(count)]
            if group > 1:
                run["Z"] = z_all
                order.append("Z")
            for kinds in ("xy", "zo", "te", "f", "v", "wu", "h", "l", "n", "s", "m"):
                order += sorted((name for name in run if name[0] in kinds), key=lambda name: (name[1:], -ord(name[0])))
        for name in order:
            run[name]()

        if not streamed:
            k_step = 2 * LANES
            n_step = 4 * LANES

            def body(i, carry):
                ns = pl.ds(pl.multiple_of(i * n_step, n_step), n_step)
                acc[:, ns] = jnp.zeros((tok, n_step), F32)

                def inner(k, carry):
                    ks = pl.ds(pl.multiple_of(k * k_step, k_step), k_step)
                    acc[:, ns] += jnp.dot(act[:, ks], wall[ks, ns], preferred_element_type=F32)
                    return carry

                lax.fori_loop(0, width // k_step, inner, 0)
                out_v[0, :, ns] = acc[:, ns].astype(BF16)
                return carry

            lax.fori_loop(0, width // n_step, body, 0)

        ended = jnp.logical_or(s == 0, s == sp - 1)

        def finish(cc):
            left(sent[cc][0], send_sem.at[0])
            if sent[cc][1]:
                left(sent[cc][1], send_sem.at[2])
            for wanted, count in ((ended, 1), (jnp.logical_not(ended), sp + 1)):
                if sp > 1:
                    @pl.when(wanted)
                    def _():
                        left(count * (rows + (chips - 1) * late_rows[cc]) * cols, send_sem.at[1])

        by_core(finish)()

        @pl.when(s < sp - 1)
        def _():
            halo_copy.wait_send()

    scratch = [
        pltpu.VMEM((tok, width), BF16),
        pltpu.VMEM((tok, width), BF16),
        pltpu.VMEM((pad, width), BF16),
        pltpu.VMEM((pad, width), BF16),
        pltpu.VMEM((pad, width), BF16),
        pltpu.VMEM((pad, width), BF16),
        pltpu.VMEM((taps, width), BF16),
        pltpu.VMEM((taps, width), F32),
        pltpu.VMEM((1, width), F32),
        pltpu.VMEM((1, width), F32),
        pltpu.VMEM((pad + tok, width), F32),
        pltpu.VMEM((tok, width), F32),
        pltpu.VMEM((tok, width), BF16),
        pltpu.VMEM((tok, width), F32),
        pltpu.VMEM((dp * rows, sp * cols), BF16),
        pltpu.SemaphoreType.DMA((5 + max(in_parts, 2),)),
        pltpu.SemaphoreType.DMA((2,)),
        pltpu.SemaphoreType.DMA((3,)),
        pltpu.SemaphoreType.DMA((2, sp)),
        pltpu.SemaphoreType.DMA((parts * (chips - 1) * 2,)),
        pltpu.SemaphoreType.DMA((chips, sp) if group == 1 else (1, 1)),
        pltpu.SemaphoreType.DMA(((parts - 1) * chips + 1,)),
    ]
    return kernel, scratch


def solution(mesh):
    sp, dp = mesh.shape["sp"], mesh.shape["dp"]
    chips = dp // 2
    xs = max(i for i in range(1, math.isqrt(chips) + 1) if chips % i == 0)
    ys = chips // xs
    parts = math.gcd(sp, max(1, 32 // dp))

    def per_device(value_half, gate_half, conv_taps, norm_gain, norm_shift, out_weight):
        _, tok, width = value_half.shape
        taps = conv_taps.shape[0]
        rows, cols = out_weight.shape
        pad = -(-(taps - 1) // 16) * 16
        kernel, scratch = make_kernel(sp, dp, xs, ys, parts, tok, width, taps, rows, cols, pad)
        return pl.pallas_call(
            kernel,
            out_shape=pltpu.VMEM(value_half.shape, BF16),
            in_specs=[pl.BlockSpec(memory_space=pltpu.HBM)] * 6,
            out_specs=pl.BlockSpec(memory_space=pltpu.VMEM),
            scratch_shapes=scratch,
            compiler_params=pltpu.CompilerParams(
                collective_id=0, has_side_effects=True, vmem_limit_bytes=VMEM_LIMIT),
        )(value_half, gate_half, conv_taps, norm_gain[None], norm_shift[None], out_weight)

    placed = (P("dp", "sp", None), P("dp", "sp", None), P(), P(), P(), P("dp", "sp"))
    return jax.shard_map(
        per_device, mesh=mesh, in_specs=placed, out_specs=P("dp", "sp", None), check_vma=False
    )
```

```python
import math
from functools import partial

import jax
import jax.numpy as jnp
from jax import lax
from jax.experimental import pallas as pl
from jax.experimental.pallas import tpu as pltpu
from jax.sharding import PartitionSpec as P

EPSILON = 1e-06
MESH = pl.DeviceIdType.MESH
F32 = jnp.float32
BF16 = jnp.bfloat16
LANES = 128
VMEM_LIMIT = 62 * 1024 * 1024
ORDER = (
    "i1", "x0", "o01", "t0", "o00", "g3", "y0", "i0", "y1", "v0", "z11", "o11", "z21", "b0", "e3", "g1",
    "g0", "z10", "g2", "a0", "z20", "f01", "e0", "o10", "f00", "v1", "s11", "z31", "w20", "v2", "f11", "e1",
    "s00", "o21", "e2", "z30", "v3", "o20", "h0", "w10", "f10", "u11", "w21", "s03", "l2", "w12", "w22", "s01",
    "u10", "w11", "l1", "l0", "l3", "o31", "n1", "n0", "m10", "w23", "o30", "s02", "m03", "s20", "m01", "f20",
    "f21", "w32", "s10", "w31", "u20", "w13", "s31", "u13", "m00", "w30", "u21", "s12", "s13", "f31", "m20", "u22",
    "f30", "w33", "s21", "u12", "m11", "m22", "s30", "m21", "u32", "s23", "u31", "m12", "m02", "u23", "s22", "m31",
    "m13", "u30", "m32", "s33", "s32", "u33", "m23", "m30", "m33",
)


def half_sigmoid(x):
    return 0.5 * jnp.tanh(0.5 * x) + 0.5


def nearest(me, count, k):
    place = jnp.int32(0)
    for here in range(count):
        there = sorted(range(count), key=lambda j: (abs(j - here), j))[k]
        place = place + jnp.where(me == here, there, 0).astype(jnp.int32)
    return place


def make_kernel(sp, dp, xs, ys, parts, tok, width, taps, rows, cols, pad):
    group = sp // parts
    part_cols = group * cols
    late_rows = [share // 8 * 8 if group == 1 else 0 for share in (rows * 7 // 32, rows * 6 // 32)]
    plane_start = (0, rows)
    half_rows, half_start = [], []
    for core_late, start, lean in zip(late_rows, plane_start, (4, 16)):
        one = (rows - core_late - (lean if core_late else 0)) // 2 // 8 * 8
        half_rows.append((one, rows - core_late - one))
        half_start.append((start + core_late, start + core_late + one))
    chips = xs * ys
    blocks = width // LANES
    row_chunk = 128 if tok % 128 == 0 else tok
    lead = pad - (taps - 1)
    in_parts = 4 if blocks % 4 == 0 else 1
    in_cols = width // in_parts
    streamed = rows % LANES == 0

    def kernel(v_hbm, g_hbm, taps_hbm, gain_hbm, shift_hbm, w_hbm, out_v,
               v_in, g_in, v_tail, g_tail, tail, halo, taps_in, taps_f, gain, shift, gated, conv, act, acc, wall,
               in_sem, halo_sem, send_sem, z_sem, recv_sem, late_sem, pair_sem):
        s = lax.axis_index("sp")
        d = lax.axis_index("dp")
        core = lax.rem(d, 2)
        x = lax.rem(d // 2, xs)
        y = d // (2 * xs)

        def index(yy, xx, cc):
            return (yy * xs + xx) * 2 + cc

        sibling = index(y, x, 1 - core)

        def along_x(step):
            return lax.rem(x + step, xs)

        def along_y(step):
            return lax.rem(y + step, ys)

        own = wall.at[pl.ds(pl.multiple_of(d * rows, rows), rows), pl.ds(pl.multiple_of(s * cols, cols), cols)]
        w_copy = pltpu.make_async_copy(w_hbm, own, in_sem.at[0])
        w_copy.start()
        tails = [
            pltpu.make_async_copy(src.at[0, pl.ds(tok - pad, pad), :], dst, in_sem.at[4])
            for src, dst in ((v_hbm, v_tail), (g_hbm, g_tail))
        ]
        for copy in tails:
            copy.start()
        loads = []
        for part in range(in_parts):
            sl = pl.ds(part * in_cols, in_cols)
            pair = (
                pltpu.make_async_copy(v_hbm.at[0, :, sl], v_in.at[:, sl], in_sem.at[5 + part]),
                pltpu.make_async_copy(g_hbm.at[0, :, sl], g_in.at[:, sl], in_sem.at[5 + part + in_parts % 4]),
            )
            loads.append(pair)
            for copy in pair:
                copy.start()
        small = [
            pltpu.make_async_copy(taps_hbm, taps_in, in_sem.at[1]),
            pltpu.make_async_copy(gain_hbm, gain, in_sem.at[2]),
            pltpu.make_async_copy(shift_hbm, shift, in_sem.at[3]),
        ]
        for copy in small:
            copy.start()

        barrier = pltpu.get_barrier_semaphore()
        friends = [(s, sibling)]
        friends += [(s, index(y, along_x(i), core)) for i in range(1, xs)]
        friends += [(s, index(along_y(i), x, core)) for i in range(1, ys)]
        for friend in friends:
            pl.semaphore_signal(barrier, inc=1, device_id=friend, device_id_type=MESH)
        above, below = s + 1 < sp, s > 0

        @pl.when(above)
        def _():
            pl.semaphore_signal(barrier, inc=1, device_id=(lax.rem(s + 1, sp), d), device_id_type=MESH)

        @pl.when(below)
        def _():
            pl.semaphore_signal(barrier, inc=1, device_id=(lax.rem(s + sp - 1, sp), d), device_id_type=MESH)

        pl.semaphore_wait(barrier, len(friends) + above.astype(jnp.int32) + below.astype(jnp.int32))
        w_copy.wait()

        me = d // 2
        sent = [[0, 0], [0, 0]]

        def by_core(act_on):
            def call(*where):
                for cc in range(2):
                    @pl.when(core == cc)
                    def _():
                        act_on(cc, *where)

            return call

        def send(cc, region, sem, target):
            copy = pltpu.make_async_remote_copy(
                src_ref=region, dst_ref=region, send_sem=send_sem.at[0], recv_sem=sem,
                device_id=(s, target), device_id_type=MESH)
            copy.start()
            sent[cc][0] += region.shape[0] * region.shape[1]

        def arrived(region, sem):
            pltpu.make_async_remote_copy(
                src_ref=region, dst_ref=region, send_sem=send_sem.at[0], recv_sem=sem,
                device_id=(s, sibling), device_id_type=MESH).wait_recv()

        def left(size, sem):
            units = size // LANES
            wide = max(j for j in range(1, blocks + 1) if units % (8 * j) == 0 and units // j <= dp * rows)
            region = wall.at[pl.ds(0, units // wide), pl.ds(0, wide * LANES)]
            pltpu.make_async_remote_copy(
                src_ref=region, dst_ref=region, send_sem=sem, recv_sem=pair_sem.at[0],
                device_id=(s, sibling), device_id_type=MESH).wait_send()

        def piece(chip, start, count, part):
            return wall.at[pl.ds(pl.multiple_of(chip * 2 * rows + start, 8), count),
                           pl.ds(pl.multiple_of(part * part_cols, part_cols), part_cols)]

        def block(cc, half, who):
            return wall.at[pl.ds(pl.multiple_of(me * 2 * rows + half_start[cc][half], 8), half_rows[cc][half]),
                           pl.ds(pl.multiple_of(who * cols, cols), cols)]

        def strip(cc, half, chip, part):
            return piece(chip, half_start[cc][half], half_rows[cc][half], part)

        def late_strip(cc, chip, who):
            return piece(chip, plane_start[cc], late_rows[cc], who)

        halo_copy = pltpu.make_async_remote_copy(
            src_ref=tail, dst_ref=halo, send_sem=halo_sem.at[0], recv_sem=halo_sem.at[1],
            device_id=(lax.rem(s + 1, sp), d), device_id_type=MESH)

        def send_halo():
            @pl.when(s < sp - 1)
            def _():
                halo_copy.start()

        def send_if(wanted, region, sem, target, column=None):
            copy = pltpu.make_async_remote_copy(
                src_ref=region, dst_ref=region, send_sem=send_sem.at[1 if column is None else 2], recv_sem=sem,
                device_id=(target, d if column is None else column), device_id_type=MESH)

            @pl.when(wanted)
            def _():
                copy.start()

        def z_sends(cc, half):
            send_if(s + 1 < sp, block(cc, half, s), z_sem.at[half, s], lax.rem(s + 1, sp))
            send_if(s > 0, block(cc, half, s), z_sem.at[half, s], lax.rem(s + sp - 1, sp))

        def z_link(k):
            source = nearest(s, sp, k)
            target = jnp.where(source < s, s + 1, s - 1)
            onward = jnp.logical_and(target >= 0, target < sp)
            return source, lax.rem(target + sp, sp), onward

        def z_forward(cc, k, half):
            source, target, onward = z_link(k)

            @pl.when(onward)
            def _():
                arrived(block(cc, half, source), z_sem.at[half, source])

            send_if(onward, block(cc, half, source), z_sem.at[half, source], target)

        def z_last(cc, k, half):
            source, _, onward = z_link(k)

            @pl.when(jnp.logical_not(onward))
            def _():
                arrived(block(cc, half, source), z_sem.at[half, source])

        my_part = s // group
        part_of = [nearest(my_part, parts, k) for k in range(parts)]

        def chip_at(fx, fy):
            return along_y(fy) * xs + along_x(fx)

        def firsts(half):
            if half == 0:
                return list(range(1, xs))
            return [xs * i for i in range(1, ys)]

        def slot(c, i, half):
            return recv_sem.at[(c * (chips - 1) + i - 1) * 2 + half]

        def pair(c, i):
            return pair_sem.at[(c - 1) * chips + i + 1 if c else 0]

        def hand_over(cc, c, i, half, j, region):
            fx, fy, tx, ty = i % xs, i // xs, j % xs, j // xs
            seen = (fy - ty) % ys * xs + (fx - tx) % xs
            send(cc, region, slot(c, seen, half), 2 * mine(j) + cc)

        def event_own(cc, c, half):
            part = part_of[c]
            if group == 1 and c > 0:
                z_last(cc, c, half)
            region = strip(cc, half, me, part)
            for j in firsts(half) + firsts(1 - half):
                hand_over(cc, c, 0, half, j, region)
            send(cc, region, pair(c, 0), sibling)

        def event_first(cc, c, half):
            for i in firsts(half):
                region = strip(cc, half, mine(i), part_of[c])
                arrived(region, slot(c, i, half))
                for j in firsts(1 - half):
                    hand_over(cc, c, i, half, j, region)
                send(cc, region, pair(c, i), sibling)

        seconds = []
        for one in range(max(xs, ys)):
            for two in range(1, max(xs, ys)):
                for half in range(2):
                    fx, fy = (one, two) if half == 0 else (two, one)
                    if fx < xs and fy < ys:
                        seconds.append((half, fx, fy))

        def event_second(cc, c, q):
            half, fx, fy = seconds[q]
            i = fy * xs + fx
            region = strip(cc, half, mine(i), part_of[c])
            arrived(region, slot(c, i, half))
            send(cc, region, pair(c, i), sibling)

        def mine(i):
            return chip_at(i % xs, i // xs)

        def late_x(cc):
            for i in range(1, xs):
                send(cc, late_strip(cc, me, s), late_sem.at[me, s], 2 * mine(i) + cc)

        def late_y(cc, c):
            for i in range(1, xs) if c else (0,):
                region, sem = late_strip(cc, mine(i), s), late_sem.at[mine(i), s]
                if i:
                    arrived(region, sem)
                for j in range(1, ys):
                    send(cc, region, sem, 2 * chip_at(0, j) + cc)

        def late_z(cc, i):
            region, sem = late_strip(cc, mine(i), s), late_sem.at[mine(i), s]
            if i >= xs:
                arrived(region, sem)
            send_if(s + 1 < sp, region, sem, lax.rem(s + 1, sp))
            send_if(s > 0, region, sem, lax.rem(s + sp - 1, sp))
            send(cc, region, pair(0, i), sibling)

        def late_forward(cc, k, i):
            source, target, onward = z_link(k)
            region, sem = late_strip(cc, mine(i), source), late_sem.at[mine(i), source]

            @pl.when(onward)
            def _():
                arrived(region, sem)

            send_if(onward, region, sem, target)
            send_if(onward, region, pair(k, i), s, sibling)

        def late_last(cc, k, i):
            source, _, onward = z_link(k)
            ended = jnp.logical_not(onward)
            region, sem = late_strip(cc, mine(i), source), late_sem.at[mine(i), source]

            @pl.when(ended)
            def _():
                arrived(region, sem)

            send_if(ended, region, pair(k, i), s, sibling)
            sent[cc][1] += region.shape[0] * region.shape[1]

        def gate_tail():
            two = pl.ds(0, 2 * pad)
            pltpu.make_async_copy(v_hbm.at[0, two, :], v_in.at[two, :], in_sem.at[4]).wait()

            def body(j, carry):
                cs = pl.ds(pl.multiple_of(j * LANES, LANES), LANES)
                tail[:, cs] = (v_tail[:, cs].astype(F32) * half_sigmoid(g_tail[:, cs].astype(F32))).astype(BF16)
                return carry

            lax.fori_loop(0, blocks, body, 0)

        def gated_rows(part):
            if in_parts == 1:
                for copy in loads[part]:
                    copy.wait()
            else:
                two = pl.ds(0, 2 * in_cols)
                pltpu.make_async_copy(v_hbm.at[0, :, two], v_in.at[:, two], in_sem.at[5 + part]).wait()

            def body(j, carry):
                cs = pl.ds(pl.multiple_of(part * in_cols + j * LANES, LANES), LANES)
                value = v_in[:, cs].astype(F32)
                gate = g_in[:, cs].astype(F32)
                gated[pl.ds(pad, tok), cs] = (value * half_sigmoid(gate)).astype(BF16).astype(F32)
                return carry

            lax.fori_loop(0, in_cols // LANES, body, 0)

        def taps_up():
            for copy in small:
                copy.wait()
            taps_f[...] = taps_in[...].astype(F32)

        def halo_rows():
            @pl.when(s == 0)
            def _():
                gated[pl.ds(0, pad), :] = jnp.zeros((pad, width), F32)

            @pl.when(s > 0)
            def _():
                halo_copy.wait_recv()

                def body(j, carry):
                    cs = pl.ds(pl.multiple_of(j * LANES, LANES), LANES)
                    gated[pl.ds(0, pad), cs] = halo[:, cs].astype(F32)
                    return carry

                lax.fori_loop(0, blocks, body, 0)

        def mix(row_starts, lo, hi):
            def body(j, carry):
                cs = pl.ds(pl.multiple_of(j * LANES, LANES), LANES)
                for start in row_starts:
                    seen = gated[pl.ds(start, row_chunk + pad), cs]
                    total = None
                    for r in range(8):
                        inner = None
                        length = row_chunk + (8 if r else 0)
                        for q in range(0, pad // 8 + 1):
                            tap = 8 * q + r - lead
                            if 0 <= tap < taps:
                                term = seen[8 * q:8 * q + length] * taps_f[pl.ds(tap, 1), cs]
                                inner = term if inner is None else inner + term
                        if inner is None:
                            continue
                        if r:
                            inner = pltpu.roll(inner, length - r, 0)[:row_chunk]
                        total = inner if total is None else total + inner
                    conv[pl.ds(start, row_chunk), cs] = total.astype(BF16).astype(F32)
                return carry

            lax.fori_loop(lo, hi, body, 0)

        def normalise(low, high):
            step = math.gcd(64, row_chunk)

            def body(i, carry):
                rs = pl.ds(pl.multiple_of(i * step, step), step)
                columns = [slice(j * LANES, (j + 1) * LANES) for j in range(blocks)]
                total = conv[rs, columns[0]]
                for cs in columns[1:]:
                    total = total + conv[rs, cs]
                mean = jnp.sum(total, axis=1, keepdims=True) * (1.0 / width)
                mean = jnp.broadcast_to(mean, (step, LANES))
                total = jnp.zeros((step, LANES), F32)
                for cs in columns:
                    centered = conv[rs, cs] - mean
                    total = total + centered * centered
                variance = jnp.sum(total, axis=1, keepdims=True) * (1.0 / width)
                scale = jnp.broadcast_to(lax.rsqrt(variance + EPSILON), (step, LANES))
                for cs in columns:
                    half = (conv[rs, cs] - mean) * scale * (0.5 * gain[:, cs]) + 0.5 * shift[:, cs]
                    act[rs, cs] = (half * jnp.tanh(half) + half).astype(BF16)
                return carry

            lax.fori_loop(low // step, high // step, body, 0)

        multiplied = [0] * parts

        def sibling_strip(cc, c, i):
            if c:
                arrived(piece(mine(i), plane_start[1 - cc], rows, part_of[c]), pair(c, i))
            elif multiplied[0] == 0:
                arrived(piece(0, 0, chips * rows, part_of[c]), pair(c, i))

        def product(c, i, start, count):
            part = part_of[c]
            ks = pl.ds(pl.multiple_of(mine(i) * 2 * rows + start, count), count)
            ns = pl.ds(pl.multiple_of(part * part_cols, part_cols), part_cols)
            return ns, jnp.dot(act[:, ks], wall[ks, ns], preferred_element_type=F32)

        def multiply(c, i, last):
            if last:
                ns, term = product(c, i, core * rows, rows)
                acc[:, ns] += term
            by_core(sibling_strip)(c, i)
            multiplied[c] += 1
            if not streamed:
                return
            ns, term = product(c, i, (1 - core) * rows, rows) if last else product(c, i, 0, 2 * rows)
            if multiplied[c] == 1:
                acc[:, ns] = term
            elif multiplied[c] < chips:
                acc[:, ns] += term
            else:
                out_v[0, :, ns] = (acc[:, ns] + term).astype(BF16)

        early = [start for start in range(0, tok, row_chunk) if start >= pad]
        late = [start for start in range(0, tok, row_chunk) if start < pad]

        edges = [blocks * i // 4 for i in range(5)]
        small_step = {
            "g": (gated_rows, in_parts),
            "e": (lambda c: mix(early, edges[c], edges[c + 1]), 4),
            "l": (lambda c: mix(late, edges[c], edges[c + 1]), 4),
            "n": (lambda c: normalise(*((late[-1] + row_chunk, tok), (0, late[-1] + row_chunk))[c]), 2),
        }
        ending = [name for name in ORDER if name[0] == "m"][-5:] if streamed and group == 1 and chips > 2 else []
        run = {
            "t0": taps_up,
            "b0": gate_tail,
            "a0": send_halo,
            "h0": halo_rows,
        }
        for kind, (act_on, count) in small_step.items():
            for c in range(count):
                run[f"{kind}{c}"] = partial(act_on, c)
        for half in range(2):
            run[f"i{half}"] = partial(by_core(z_sends), half)
            if group == 1:
                for k in range(1, sp):
                    run[f"z{k}{half}"] = partial(by_core(z_forward), k, half)
        for c in range(parts):
            for half in range(2):
                run[f"o{c}{half}"] = partial(by_core(event_own), c, half)
                run[f"f{c}{half}"] = partial(by_core(event_first), c, half)
            for q in range(len(seconds)):
                run[f"s{c}{q}"] = partial(by_core(event_second), c, q)
            for i in range(chips):
                run[f"m{c}{i}"] = partial(multiply, c, i, f"m{c}{i}" in ending)
        if group == 1:
            run["x0"] = by_core(late_x)
            run["y0"] = partial(by_core(late_y), 0)
            run["y1"] = partial(by_core(late_y), 1)
            for i in range(chips):
                run[f"v{i}"] = partial(by_core(late_z), i)
                for k in range(1, sp):
                    run[f"w{k}{i}"] = partial(by_core(late_forward), k, i)
                    run[f"u{k}{i}"] = partial(by_core(late_last), k, i)

        def z_all():
            for k in range(1, sp):
                for half in range(2):
                    by_core(z_forward)(k, half)
                for half in range(2):
                    by_core(z_last)(k, half)

        order = [name for name in ORDER if name in run]
        if len(order) < len(run):
            order = [f"{kind}{c}" for kind, count in (("i", 2), ("b", 1), ("g", in_parts), ("a", 1)) for c in range(count)]
            if group > 1:
                run["Z"] = z_all
                order.append("Z")
            for kinds in ("xy", "zo", "te", "f", "v", "wu", "h", "l", "n", "s", "m"):
                order += sorted((name for name in run if name[0] in kinds), key=lambda name: (name[1:], -ord(name[0])))
        for name in order:
            run[name]()

        if not streamed:
            k_step = 2 * LANES
            n_step = 4 * LANES

            def body(i, carry):
                ns = pl.ds(pl.multiple_of(i * n_step, n_step), n_step)
                acc[:, ns] = jnp.zeros((tok, n_step), F32)

                def inner(k, carry):
                    ks = pl.ds(pl.multiple_of(k * k_step, k_step), k_step)
                    acc[:, ns] += jnp.dot(act[:, ks], wall[ks, ns], preferred_element_type=F32)
                    return carry

                lax.fori_loop(0, width // k_step, inner, 0)
                out_v[0, :, ns] = acc[:, ns].astype(BF16)
                return carry

            lax.fori_loop(0, width // n_step, body, 0)

        ended = jnp.logical_or(s == 0, s == sp - 1)

        def finish(cc):
            left(sent[cc][0], send_sem.at[0])
            if sent[cc][1]:
                left(sent[cc][1], send_sem.at[2])
            for wanted, count in ((ended, 1), (jnp.logical_not(ended), sp + 1)):
                if sp > 1:
                    @pl.when(wanted)
                    def _():
                        left(count * (rows + (chips - 1) * late_rows[cc]) * cols, send_sem.at[1])

        by_core(finish)()

        @pl.when(s < sp - 1)
        def _():
            halo_copy.wait_send()

    scratch = [
        pltpu.VMEM((tok, width), BF16),
        pltpu.VMEM((tok, width), BF16),
        pltpu.VMEM((pad, width), BF16),
        pltpu.VMEM((pad, width), BF16),
        pltpu.VMEM((pad, width), BF16),
        pltpu.VMEM((pad, width), BF16),
        pltpu.VMEM((taps, width), BF16),
        pltpu.VMEM((taps, width), F32),
        pltpu.VMEM((1, width), F32),
        pltpu.VMEM((1, width), F32),
        pltpu.VMEM((pad + tok, width), F32),
        pltpu.VMEM((tok, width), F32),
        pltpu.VMEM((tok, width), BF16),
        pltpu.VMEM((tok, width), F32),
        pltpu.VMEM((dp * rows, sp * cols), BF16),
        pltpu.SemaphoreType.DMA((5 + max(in_parts, 2),)),
        pltpu.SemaphoreType.DMA((2,)),
        pltpu.SemaphoreType.DMA((3,)),
        pltpu.SemaphoreType.DMA((2, sp)),
        pltpu.SemaphoreType.DMA((parts * (chips - 1) * 2,)),
        pltpu.SemaphoreType.DMA((chips, sp) if group == 1 else (1, 1)),
        pltpu.SemaphoreType.DMA(((parts - 1) * chips + 1,)),
    ]
    return kernel, scratch


def solution(mesh):
    sp, dp = mesh.shape["sp"], mesh.shape["dp"]
    chips = dp // 2
    xs = max(i for i in range(1, math.isqrt(chips) + 1) if chips % i == 0)
    ys = chips // xs
    parts = math.gcd(sp, max(1, 32 // dp))

    def per_device(value_half, gate_half, conv_taps, norm_gain, norm_shift, out_weight):
        _, tok, width = value_half.shape
        taps = conv_taps.shape[0]
        rows, cols = out_weight.shape
        pad = -(-(taps - 1) // 16) * 16
        kernel, scratch = make_kernel(sp, dp, xs, ys, parts, tok, width, taps, rows, cols, pad)
        return pl.pallas_call(
            kernel,
            out_shape=pltpu.VMEM(value_half.shape, BF16),
            in_specs=[pl.BlockSpec(memory_space=pltpu.HBM)] * 6,
            out_specs=pl.BlockSpec(memory_space=pltpu.VMEM),
            scratch_shapes=scratch,
            compiler_params=pltpu.CompilerParams(
                collective_id=0, has_side_effects=True, vmem_limit_bytes=VMEM_LIMIT),
        )(value_half, gate_half, conv_taps, norm_gain[None], norm_shift[None], out_weight)

    placed = (P("dp", "sp", None), P("dp", "sp", None), P(), P(), P(), P("dp", "sp"))
    return jax.shard_map(
        per_device, mesh=mesh, in_specs=placed, out_specs=P("dp", "sp", None), check_vma=False
    )
```
